32 devices in a mesh: fs: 8 (over z, y), tp: 4 (over x, core).
Axes of the slice: x: 2, y: 2, z: 4, core: 2. Of those that a mesh axis runs over, the one named last changes fastest.
Arguments:
- tokens: bfloat16 [1024, 2048], P('fs', 'tp'), may hold values from -6 to 6
- routes: int32 [1024, 2], P('fs'), may hold values from 0 to 7, all different within a row; in each aligned block of 128 rows (0 to 127, 128 to 255, ...) at most 48 rows name the same one
- route_weight: float32 [1024, 2], P('fs'), may hold values from 0.05 to 1
- gain: float32 [2048], P('fs'), may hold values from 0.1 to 1.9
- gate_weight: float32 [8, 2048, 512], P(None, 'fs', 'tp'), may hold values from -0.125 to 0.125
- up_weight: float32 [8, 2048, 512], P(None, 'fs', 'tp'), may hold values from -0.125 to 0.125
- down_weight: float32 [8, 512, 2048], P(None, 'tp', 'fs'), may hold values from -0.25 to 0.25
Outputs:
- gate_out: bfloat16 [8, 2048, 512], P('fs', None, 'tp')
- up_out: bfloat16 [8, 2048, 512], P('fs', None, 'tp')
- down_out: bfloat16 [8, 512, 2048], P('fs', 'tp')
- mixed: bfloat16 [1024, 2048], P('fs', 'tp')
The draws below stay inside these ranges and needn't reach their ends.
Inputs may be any that keep to these rules, and one draw needn't show every extreme that they name: `routes`: each row names 2 different experts. Among the rows of one index of fs (aligned blocks of 128 rows) no expert is named more than 48 times, a bound that some block reaches.
All inputs are finite; a program needn't handle non-finite values.
Results may differ from the reference program's by a relative error of at most 0.0095.
Values may be sent and summed in bfloat16 or wider, within the bound.
A program may use at most 64 MiB of HBM per device.

```python
import math
import jax
import jax.numpy as jnp
import numpy as np
from jax import lax

D = 2048
F = 512
TOP = 2
TOK_DEV = 128
EXPERTS = 8
CAP = 48
TOKENS = 1024
N_FS = 8
N_TP = 4


def block_scale(rng, shape, cuts, smallest, high):
    loudness = 1.0
    for dim, blocks in cuts:
        heights = jax.random.uniform(jax.random.fold_in(jax.random.fold_in(rng, 6), dim), (blocks,), jnp.float32, smallest / len(cuts), high / len(cuts))
        loudness = loudness * jnp.repeat(jnp.exp(heights), shape[dim] // blocks).reshape((-1,) + (1,) * (len(shape) - 1 - dim))
    return loudness


def shared_out(own_key, own, number, rows, count, top, limit, lean):
    sequence = jax.random.permutation(own_key, count)
    heavy_load, usual = shares(count, rows * top, limit, lean, True), shares(count, rows * top, limit, lean, False)
    places = jnp.arange(count)

    def named(sizes, rotation):
        used = int((sizes > 0).sum())
        fixed = max(1, used // 4)
        moved = fixed + (places - fixed + rotation * (used - fixed)) % max(1, count - fixed)
        return jnp.zeros((count,), jnp.int32).at[sequence[jnp.where(places < fixed, places, moved)]].set(jnp.asarray(sizes, jnp.int32))

    sizes = jnp.where(number % 4 == 0, named(heavy_load, number // 4), named(usual, number - number // 4 - 1))
    mixed = jax.random.permutation(jax.random.fold_in(own, 3), count)
    source_of, taker = mixed[0:count // 2 * 2:2], mixed[1:count // 2 * 2:2]
    slack = jnp.minimum(sizes[source_of] - 1, limit - sizes[taker]) // 2
    slack = jnp.where((source_of == sequence[0]) | (taker == sequence[0]) | (sizes[taker] == 0), 0, jnp.maximum(slack, 0))
    moved = jax.random.randint(jax.random.fold_in(own, 4), (count // 2,), 0, 1 << 20) % (slack + 1)
    sizes = sizes.at[source_of].add(-moved).at[taker].add(moved)
    members = jnp.searchsorted(jnp.cumsum(sizes), jnp.arange(rows * top), side="right").astype(jnp.int32)
    table = members.reshape(top, rows).T
    table = table[jax.random.permutation(jax.random.fold_in(own, 1), rows)]
    rotation = jax.random.randint(jax.random.fold_in(own, 2), (rows, 1), 0, top)
    return jnp.take_along_axis(table, (jnp.arange(top)[None, :] + rotation) % top, axis=1)


def shares(amount, total, limit, skew, full):
    weights = [(1 << 20) // math.isqrt(standing ** skew) + 1 for standing in range(1, amount + 1)]
    largest = limit if full else min(limit, max(-(-total // amount), total * weights[0] // sum(weights)))
    least = 1 if total - largest >= amount - 1 else 0
    holding, spare = [largest] + [least] * (amount - 1), total - largest - least * (amount - 1)
    while spare > 0:
        movable = [i for i in range(1, amount) if holding[i] < largest] or [i for i in range(1, amount) if holding[i] < limit]
        mass, remaining = sum([weights[i] for i in movable]), spare
        for i in movable:
            extra = min(limit - holding[i], max(1, remaining * weights[i] // mass), spare)
            holding[i] = holding[i] + extra
            spare = spare - extra
    return np.array(holding)


def gaussian(own_key, dims, width, limit, split=(), kind=jnp.bfloat16):
    factor_of = block_scale(own_key, dims, split, -0.22, 0.18) if split else 1.0
    entries = jax.random.normal(own_key, dims, jnp.float32) * width * factor_of
    return jnp.minimum(jnp.maximum(entries, -limit), limit).astype(kind)


def setup_inputs(seed: int = 0) -> dict:
    seeds = jax.random.split(jax.random.key(seed), 8)
    tokens = gaussian(seeds[0], (TOKENS, D), 1.0, 6.0, ((0, 8), (1, 4)))
    routes_keys = jax.random.split(jax.random.fold_in(seeds[1], 1), TOKENS // TOK_DEV)
    routes_turns = jax.random.permutation(jax.random.fold_in(seeds[1], 3), TOKENS // TOK_DEV)
    routes = jax.vmap(lambda own, number: shared_out(jax.random.fold_in(seeds[1], 2), own, number, TOK_DEV, EXPERTS, TOP, CAP, 2))(routes_keys, routes_turns).reshape((TOKENS, TOP))
    route_weight = jnp.clip(0.05 + 0.95 * jax.random.uniform(seeds[2], (TOKENS, TOP), jnp.float32) ** block_scale(seeds[2], (TOKENS, TOP), ((0, 8),), -0.2, 0.2), 0.05, 1.0)
    gain = jnp.clip(1.0 + 0.18 * jax.random.normal(seeds[3], (D,), jnp.float32), 0.1, 1.9)
    gate_weight = gaussian(seeds[4], (EXPERTS, D, F), D ** -0.5, 0.125, ((1, 8), (2, 4)), jnp.float32)
    up_weight = gaussian(seeds[5], (EXPERTS, D, F), D ** -0.5, 0.125, ((1, 8), (2, 4)), jnp.float32)
    down_weight = gaussian(seeds[6], (EXPERTS, F, D), F ** -0.5, 0.25, ((1, 4), (2, 8)), jnp.float32)
    return dict(tokens=tokens, routes=routes, route_weight=route_weight, gain=gain, gate_weight=gate_weight, up_weight=up_weight, down_weight=down_weight)


def reference(tokens, routes, route_weight, gain, gate_weight, up_weight, down_weight):
    gate_out = (gain[None, :, None] * gate_weight).astype(jnp.bfloat16)
    up_out = (gain[None, :, None] * up_weight).astype(jnp.bfloat16)
    down_out = down_weight.astype(jnp.bfloat16)
    values = tokens.astype(jnp.float32)
    normed = (values * lax.rsqrt(lax.optimization_barrier(jnp.mean(values * values, axis=-1, keepdims=True)) + 1e-06)).astype(jnp.bfloat16)
    blocks = routes.reshape(N_FS, TOK_DEV * TOP)
    hits = (blocks[:, :, None] == jnp.arange(EXPERTS, dtype=jnp.int32)[None, None, :]).astype(jnp.int32)
    ranks = lax.optimization_barrier(jnp.sum((jnp.cumsum(hits, axis=1) - 1) * hits, axis=2))
    homes = jnp.arange(N_FS, dtype=jnp.int32)[:, None]
    position = (blocks * (N_FS * CAP) + homes * CAP + ranks).reshape(-1).astype(jnp.int32)
    count = TOKENS * TOP
    source = jnp.full((EXPERTS * N_FS * CAP,), count, jnp.int32)
    source = source.at[position].set(jnp.arange(count, dtype=jnp.int32)).reshape(EXPERTS, N_FS * CAP)
    unit = F // N_TP

    def per_expert(items):
        src, w_gate, w_up, w_down = items
        rows = normed[jnp.minimum(src // TOP, TOKENS - 1)]
        rows = jnp.where((src < count)[:, None], rows, jnp.zeros_like(rows))
        gate_act = jnp.dot(rows, w_gate, preferred_element_type=jnp.float32)
        up_act = jnp.dot(rows, w_up, preferred_element_type=jnp.float32)
        hidden = (jax.nn.silu(gate_act) * up_act).astype(jnp.bfloat16)
        pieces = []
        for block in range(N_TP):
            part = jnp.dot(hidden[:, block * unit:(block + 1) * unit], w_down[block * unit:(block + 1) * unit], preferred_element_type=jnp.float32).astype(jnp.bfloat16)
            pieces.append(part.astype(jnp.float32))
        return lax.optimization_barrier(jnp.sum(jnp.stack(pieces), axis=0)).astype(jnp.bfloat16)
    results = lax.map(per_expert, (source, gate_out, up_out, down_out))
    picked = results.reshape(EXPERTS * N_FS * CAP, D)[position].astype(jnp.float32).reshape(TOKENS, TOP, D)
    share = route_weight / lax.optimization_barrier(jnp.sum(route_weight, axis=1, keepdims=True))
    mixed = lax.optimization_barrier(jnp.sum(share[:, :, None] * picked, axis=1)).astype(jnp.bfloat16)
    return (gate_out, up_out, down_out, mixed)
```

```python
import functools

import jax
import jax.numpy as jnp
from jax import lax
from jax.experimental import pallas as pl
from jax.experimental.pallas import tpu as pltpu
from jax.sharding import PartitionSpec as P


def normalize(rows):
    values = rows.astype(jnp.float32)
    return (values * lax.rsqrt(jnp.mean(values * values, axis=-1, keepdims=True) + 1e-06)).astype(
        jnp.bfloat16
    )


def local(tokens, routes, route_weight, gain, gate_weight, up_weight, down_weight):
    fs_count = lax.axis_size("fs")
    tp_count = lax.axis_size("tp")
    gain_rows = gain[None, :, None]
    gate_new = (gain_rows * gate_weight).astype(jnp.bfloat16)
    up_new = (gain_rows * up_weight).astype(jnp.bfloat16)
    gate_out, up_out = (
        lax.all_to_all(gate_new, "fs", split_axis=0, concat_axis=1, tiled=True),
        lax.all_to_all(up_new, "fs", split_axis=0, concat_axis=1, tiled=True),
    )
    down_out = lax.all_to_all(
        down_weight.astype(jnp.bfloat16), "fs", split_axis=0, concat_axis=2, tiled=True
    )
    tok_rows, top = routes.shape
    capacity = min(tok_rows, max(2, 3 * tok_rows * top // (2 * fs_count)))
    flat = routes.reshape(-1)
    count = flat.shape[0]
    hits = (flat[:, None] == jnp.arange(fs_count, dtype=jnp.int32)[None, :]).astype(jnp.int32)
    ranks = jnp.sum((jnp.cumsum(hits, axis=0) - 1) * hits, axis=1)
    slots = flat * capacity + ranks
    source = jnp.full((fs_count * capacity,), count, jnp.int32)
    source = source.at[slots].set(jnp.arange(count, dtype=jnp.int32))
    filled = (source < count)[:, None]
    row_of = jnp.minimum(source // top, tok_rows - 1)
    whole = lax.all_gather(tokens, "tp", axis=1, tiled=True)
    normed = normalize(whole)
    packed = jnp.where(filled, normed[row_of], jnp.zeros((), jnp.bfloat16))
    arrived = lax.all_to_all(
        packed.reshape(fs_count, capacity, -1), "fs", split_axis=0, concat_axis=0, tiled=True
    )
    arrived = arrived.reshape(fs_count * capacity, -1)
    gate_act = jnp.dot(arrived, gate_out[0], preferred_element_type=jnp.float32)
    up_act = jnp.dot(arrived, up_out[0], preferred_element_type=jnp.float32)
    hidden = (jax.nn.silu(gate_act) * up_act).astype(jnp.bfloat16)
    slot_rows = hidden.shape[0]
    unit_rows = down_out.shape[1]
    hidden_all = lax.all_gather(hidden, "tp", axis=1, tiled=True)
    column_block = lax.all_to_all(
        down_out[0].reshape(unit_rows, tp_count, -1), "tp", split_axis=1, concat_axis=0, tiled=True
    )
    column_block = column_block.reshape(tp_count, unit_rows, -1)
    hidden_blocks = hidden_all.reshape(slot_rows, tp_count, unit_rows)
    partial_value = jnp.einsum(
        "sju,jud->sjd", hidden_blocks, column_block, preferred_element_type=jnp.float32
    ).astype(jnp.bfloat16)
    expert_out = jnp.sum(partial_value, axis=1, dtype=jnp.float32).astype(jnp.bfloat16)
    returned = lax.all_to_all(
        expert_out.reshape(fs_count, capacity, -1), "fs", split_axis=0, concat_axis=0, tiled=True
    )
    returned = returned.reshape(fs_count * capacity, -1)
    picked = returned[slots].reshape(tok_rows, top, -1)
    share = route_weight / jnp.sum(route_weight, axis=1, keepdims=True)
    mixed = jnp.sum(share[:, :, None] * picked.astype(jnp.float32), axis=1).astype(jnp.bfloat16)
    return (gate_out, up_out, down_out, mixed)


MESH = pl.DeviceIdType.MESH
VMEM_BYTES = 67043328


def flip(index, mask):
    other = index
    bit = 1
    while bit <= mask:
        if mask & bit:
            other = other + (1 - 2 * lax.rem(lax.div(index, bit), 2)) * bit
        bit *= 2
    return other


def serve_kernel(
    fs, tp, cap,
    routes_ref, rw_ref, gain_ref, tokens_hbm, gw_hbm, uw_hbm, dw_hbm,
    gat, upw, dn, r, picks_ref, share_ref,
    tokens_ref, gw, uw, dw, gsend, usend, dsend,
    psend, x, n, h, wd, y,
    load_sem,
    w_s, w_r, p_s, p_r, xf_s, xf_r, h_s, h_r, wd_s, wd_r, y_s, y_r, own_sem,
):
    me = lax.axis_index("fs")
    mt = lax.axis_index("tp")
    toks, cols = tokens_ref.shape
    rows = gw.shape[1]
    units = gw.shape[2]
    each = cols // rows
    slots = fs * cap
    side = lax.div(me, fs // 2)
    order = [i for k in range(fs // 2) for i in (fs - 1 - k, fs // 2 - 1 - k) if i]
    near = [i for i in order if i < fs // 2]
    far = [i for i in order if i >= fs // 2]
    torder = list(range(1, tp))

    loads = [
        pltpu.make_async_copy(src, dst, load_sem.at[k])
        for k, (src, dst) in enumerate(
            ((gw_hbm, gw), (uw_hbm, uw), (dw_hbm, dw), (tokens_hbm, tokens_ref))
        )
    ]
    for load in loads[3:] + loads[:3]:
        load.start()

    barrier = pltpu.get_barrier_semaphore()
    for i in range(fs):
        for j in range(tp):
            if i or j:
                pl.semaphore_signal(
                    barrier, inc=1, device_id=(flip(me, i), flip(mt, j)), device_id_type=MESH
                )

    first, second = routes_ref[0:1, :], routes_ref[1:2, :]
    expert = lax.broadcasted_iota(jnp.int32, (fs, toks), 0)
    member = (expert == first) | (expert == second)
    earlier = lax.broadcasted_iota(jnp.int32, (toks, toks), 0) < lax.broadcasted_iota(
        jnp.int32, (toks, toks), 1
    )
    rank = jnp.dot(
        jnp.where(member, 1.0, 0.0).astype(jnp.bfloat16),
        jnp.where(earlier, 1.0, 0.0).astype(jnp.bfloat16),
        preferred_element_type=jnp.float32,
    )
    rank = jnp.where(member, rank, -1.0)
    place = lax.broadcasted_iota(jnp.int32, (cap, toks), 0).astype(jnp.float32)
    loads[3].wait()
    tokens = tokens_ref[...]
    hits = []
    for e in range(fs):
        hit = jnp.where(place == rank[e:e + 1, :], 1.0, 0.0)
        psend[e] = jnp.dot(
            hit.astype(jnp.bfloat16), tokens, preferred_element_type=jnp.float32
        ).astype(jnp.bfloat16)
        hits.append(hit)
    x[mt, me] = psend[me]

    pl.semaphore_wait(barrier, fs * tp - 1)

    sends = []

    def send(src, dst, s, d, device):
        copy = pltpu.make_async_remote_copy(
            src_ref=src, dst_ref=dst, send_sem=s, recv_sem=d, device_id=device, device_id_type=MESH
        )
        copy.start()
        sends.append(copy)
        return copy

    dispatched = {}
    for i in order:
        peer = flip(me, i)
        dispatched[i] = send(psend.at[peer], x.at[mt, me], p_s.at[i], p_r.at[i], (peer, mt))

    gain = jnp.broadcast_to(gain_ref[...], (units, rows)).T
    placed = {}
    owns = []
    for k, (raw, buf, dst) in enumerate(((gw, gsend, gat), (uw, usend, upw), (dw, dsend, dn))):
        loads[k].wait()
        for e in range(fs):
            buf[e] = (gain * raw[e] if k < 2 else raw[e]).astype(jnp.bfloat16)
        for i in order if k < 2 else near + far:
            peer = flip(me, i)
            target = dst.at[me] if k < 2 else dst.at[:, pl.ds(pl.multiple_of(me * rows, rows), rows)]
            placed[k, i] = send(buf.at[peer], target, w_s.at[k, i], w_r.at[k, i], (peer, mt))
        target = dst.at[me] if k < 2 else dst.at[:, pl.ds(pl.multiple_of(me * rows, rows), rows)]
        own = pltpu.make_async_copy(buf.at[me], target, own_sem.at[k])
        own.start()
        owns.append(own)
        if k == 0:
            forwards = []
            for j in torder:
                forwards.append(
                    send(x.at[mt, me], x.at[mt, me], xf_s.at[0, j], xf_r.at[0, j], (me, flip(mt, j)))
                )

    for i in reversed(order):
        dispatched[i].wait_recv()
        peer = flip(me, i)
        for j in torder:
            forwards.append(
                send(x.at[mt, peer], x.at[mt, peer], xf_s.at[i, j], xf_r.at[i, j], (me, flip(mt, j)))
            )
    for k, named in enumerate((first, second)):
        picked = jnp.concatenate([jnp.where(named == e, hits[e], 0.0) for e in range(fs)], axis=0)
        picks_ref[k] = picked.T.astype(jnp.bfloat16)
        weight = rw_ref[k:k + 1, :] / (rw_ref[0:1, :] + rw_ref[1:2, :])
        share_ref[k] = jnp.broadcast_to(weight, (toks, toks)).T

    for copy in forwards:
        copy.wait_recv()

    for s in range(fs):
        total = jnp.zeros((cap, 1), jnp.float32)
        for j in range(tp):
            value = x[j, s].astype(jnp.float32)
            total = total + jnp.sum(value * value, axis=-1, keepdims=True)
        scale = lax.rsqrt(total / (tp * cols) + 1e-06)
        for j in range(tp):
            normed = (x[j, s].astype(jnp.float32) * scale).astype(jnp.bfloat16)
            for part in range(each):
                n[j * each + part, s * cap:(s + 1) * cap] = normed[:, part * rows:(part + 1) * rows]

    acts = []
    for k, dst in enumerate((gat, upw)):
        act = jnp.zeros((slots, units), jnp.float32)
        for i in [0] + order:
            if i == 0:
                owns[k].wait()
            else:
                placed[k, i].wait_recv()
            piece = flip(me, i)
            act = act + jnp.dot(n[piece], dst[piece], preferred_element_type=jnp.float32)
        acts.append(act)
    hidden = acts[0] / (1.0 + jnp.exp(-acts[0])) * acts[1]
    h[mt] = hidden.astype(jnp.bfloat16)
    shared = [send(h.at[mt], h.at[mt], h_s.at[j], h_r.at[j], (me, flip(mt, j))) for j in torder]

    moves = []

    def gather(masks):
        for i in masks:
            if i == 0:
                owns[2].wait()
            else:
                placed[2, i].wait_recv()
            piece = flip(me, i)
            owner, part = lax.rem(piece, tp), lax.div(piece, tp)
            block = dn.at[:, pl.ds(pl.multiple_of(piece * rows, rows), rows)]
            stays = pltpu.make_async_copy(block, wd.at[mt, part], wd_r.at[mt, part])
            goes = pltpu.make_async_remote_copy(
                src_ref=block, dst_ref=wd.at[mt, part], send_sem=wd_s.at[i],
                recv_sem=wd_r.at[mt, part], device_id=(me, owner), device_id_type=MESH,
            )
            pl.when(owner == mt)(stays.start)
            pl.when(owner != mt)(goes.start)
            moves.append((owner != mt, goes))

    def give_back(late):
        for q in range(each // 2):
            part = (1 - side if late else side) * (each // 2) + q
            for j in range(tp):
                pltpu.make_async_copy(wd.at[j, part], wd.at[j, part], wd_r.at[j, part]).wait()
            result = jnp.zeros((slots, rows), jnp.float32)
            for j in range(tp):
                term = jnp.dot(h[j], wd[j, part], preferred_element_type=jnp.float32)
                result = result + term.astype(jnp.bfloat16).astype(jnp.float32)
            v = late * (each // 2) + q
            y[v] = result.astype(jnp.bfloat16).reshape(fs, cap, rows)
            piece = part * tp + mt
            home, slot = lax.div(piece, each), lax.rem(piece, each)
            for i in order:
                peer = flip(me, i)
                send(y.at[v, peer], r.at[slot, me], y_s.at[v, i], y_r.at[i, slot], (peer, home))
            stays = pltpu.make_async_copy(y.at[v, me], r.at[slot, me], y_r.at[0, slot])
            goes = pltpu.make_async_remote_copy(
                src_ref=y.at[v, me], dst_ref=r.at[slot, me], send_sem=y_s.at[v, 0],
                recv_sem=y_r.at[0, slot], device_id=(me, home), device_id_type=MESH,
            )
            pl.when(home == mt)(stays.start)
            pl.when(home != mt)(goes.start)
            moves.append((home != mt, goes))

    gather([0] + near)
    for copy in shared:
        copy.wait_recv()
    give_back(0)
    gather(far)
    give_back(1)

    for i in [0] + order:
        for slot in range(each):
            landed = r.at[slot, flip(me, i)]
            pltpu.make_async_copy(landed, landed, y_r.at[i, slot]).wait()
    for copy in sends:
        copy.wait_send()
    for away, goes in moves:
        pl.when(away)(goes.wait_send)


def mix_kernel(gat, upw, dn, r, picks_ref, share_ref, gate_hbm, up_hbm, down_hbm, mixed_hbm, mixed, sem):
    outs = [
        pltpu.make_async_copy(src, dst, sem.at[k])
        for k, (src, dst) in enumerate(
            ((gat, gate_hbm), (upw, up_hbm), (dn, down_hbm), (mixed, mixed_hbm))
        )
    ]
    for copy in outs[:3]:
        copy.start()
    each, fs, cap, rows = r.shape
    for slot in range(each):
        back = r[slot].reshape(fs * cap, rows)
        total = jnp.zeros((mixed.shape[0], rows), jnp.float32)
        for k in range(2):
            term = jnp.dot(picks_ref[k], back, preferred_element_type=jnp.float32)
            total = total + share_ref[k][:, 0:1] * term
        mixed[:, slot * rows:(slot + 1) * rows] = total.astype(jnp.bfloat16)
    outs[3].start()
    for copy in outs:
        copy.wait()


def fused(tokens, routes, route_weight, gain, gate_weight, up_weight, down_weight):
    fs = lax.axis_size("fs")
    tp = lax.axis_size("tp")
    toks, cols = tokens.shape
    top = routes.shape[1]
    cap = capacity_of(toks, top, fs)
    rows, units = gate_weight.shape[1:]
    each = cols // rows
    slots = fs * cap
    bf, f32 = jnp.bfloat16, jnp.float32
    hbm, vmem = pl.BlockSpec(memory_space=pltpu.HBM), pl.BlockSpec(memory_space=pltpu.VMEM)
    dma = pltpu.SemaphoreType.DMA
    kept = 2 * (3 * fs * rows * units + slots * cols + top * toks * slots) + 4 * top * toks * toks
    landed = pl.pallas_call(
        functools.partial(serve_kernel, fs, tp, cap),
        out_shape=(
            pltpu.VMEM((fs, rows, units), bf),
            pltpu.VMEM((fs, rows, units), bf),
            pltpu.VMEM((units, fs * rows), bf),
            pltpu.VMEM((each, fs, cap, rows), bf),
            pltpu.VMEM((top, toks, slots), bf),
            pltpu.VMEM((top, toks, toks), f32),
        ),
        in_specs=[vmem] * 3 + [hbm] * 4,
        out_specs=(vmem,) * 6,
        scratch_shapes=[
            pltpu.VMEM((toks, cols), bf),
            pltpu.VMEM((fs, rows, units), f32),
            pltpu.VMEM((fs, rows, units), f32),
            pltpu.VMEM((fs, units, rows), f32),
            pltpu.VMEM((fs, rows, units), bf),
            pltpu.VMEM((fs, rows, units), bf),
            pltpu.VMEM((fs, units, rows), bf),
            pltpu.VMEM((fs, cap, cols), bf),
            pltpu.VMEM((tp, fs, cap, cols), bf),
            pltpu.VMEM((fs, slots, rows), bf),
            pltpu.VMEM((tp, slots, units), bf),
            pltpu.VMEM((tp, each, units, rows), bf),
            pltpu.VMEM((each, fs, cap, rows), bf),
            dma((4,)),
            dma((3, fs)), dma((3, fs)), dma((fs,)), dma((fs,)),
            dma((fs, tp)), dma((fs, tp)), dma((tp,)), dma((tp,)),
            dma((fs,)), dma((tp, each)), dma((each, fs)), dma((fs, each)), dma((3,)),
        ],
        compiler_params=pltpu.CompilerParams(
            collective_id=0, has_side_effects=True, vmem_limit_bytes=VMEM_BYTES - kept - 2**16
        ),
        name="serve",
    )(routes.T, route_weight.T, gain.reshape(1, -1), tokens, gate_weight, up_weight, down_weight)
    gate, up, down, mixed = pl.pallas_call(
        mix_kernel,
        out_shape=(
            jax.ShapeDtypeStruct((fs, rows, units), bf),
            jax.ShapeDtypeStruct((fs, rows, units), bf),
            jax.ShapeDtypeStruct((units, fs * rows), bf),
            jax.ShapeDtypeStruct((toks, cols), bf),
        ),
        in_specs=[vmem] * 6,
        out_specs=(hbm,) * 4,
        scratch_shapes=[pltpu.VMEM((toks, cols), bf), dma((4,))],
        compiler_params=pltpu.CompilerParams(vmem_limit_bytes=16 * 2**20),
        name="mix",
    )(*landed)
    return (
        gate.reshape(1, fs * rows, units),
        up.reshape(1, fs * rows, units),
        down[None],
        mixed,
    )


def capacity_of(tok_rows, top, fs_count):
    return min(tok_rows, max(2, 3 * tok_rows * top // (2 * fs_count)))


def one_kernel(fs, tp, toks, top, experts, rows, units, cols):
    cap = capacity_of(toks, top, fs)
    powers = fs & (fs - 1) == 0 and tp & (tp - 1) == 0
    small = fs <= 16 and tp <= 8 and top == 2 and experts == fs
    tiled = cap % 16 == 0 and rows % 128 == 0 and units % 128 == 0 and toks % 128 == 0
    return powers and small and tiled and cols % (2 * rows) == 0 and fs * rows == tp * cols


def program(*args):
    tokens, routes, gate_weight = args[0], args[1], args[4]
    experts, rows, units = gate_weight.shape
    if one_kernel(
        lax.axis_size("fs"), lax.axis_size("tp"), tokens.shape[0], routes.shape[1],
        experts, rows, units, tokens.shape[1],
    ):
        return fused(*args)
    return local(*args)


def solution(mesh):
    in_specs = (
        P("fs", "tp"),
        P("fs", None),
        P("fs", None),
        P("fs"),
        P(None, "fs", "tp"),
        P(None, "fs", "tp"),
        P(None, "tp", "fs"),
    )
    out_specs = (P("fs", None, "tp"), P("fs", None, "tp"), P("fs", "tp", None), P("fs", "tp"))
    return jax.shard_map(program, mesh=mesh, in_specs=in_specs, out_specs=out_specs, check_vma=False)
```

```python
import functools

import jax
import jax.numpy as jnp
from jax import lax
from jax.experimental import pallas as pl
from jax.experimental.pallas import tpu as pltpu
from jax.sharding import PartitionSpec as P


def normalize(rows):
    values = rows.astype(jnp.float32)
    return (values * lax.rsqrt(jnp.mean(values * values, axis=-1, keepdims=True) + 1e-06)).astype(
        jnp.bfloat16
    )


def local(tokens, routes, route_weight, gain, gate_weight, up_weight, down_weight):
    fs_count = lax.axis_size("fs")
    tp_count = lax.axis_size("tp")
    gain_rows = gain[None, :, None]
    gate_new = (gain_rows * gate_weight).astype(jnp.bfloat16)
    up_new = (gain_rows * up_weight).astype(jnp.bfloat16)
    gate_out, up_out = (
        lax.all_to_all(gate_new, "fs", split_axis=0, concat_axis=1, tiled=True),
        lax.all_to_all(up_new, "fs", split_axis=0, concat_axis=1, tiled=True),
    )
    down_out = lax.all_to_all(
        down_weight.astype(jnp.bfloat16), "fs", split_axis=0, concat_axis=2, tiled=True
    )
    tok_rows, top = routes.shape
    capacity = min(tok_rows, max(2, 3 * tok_rows * top // (2 * fs_count)))
    flat = routes.reshape(-1)
    count = flat.shape[0]
    hits = (flat[:, None] == jnp.arange(fs_count, dtype=jnp.int32)[None, :]).astype(jnp.int32)
    ranks = jnp.sum((jnp.cumsum(hits, axis=0) - 1) * hits, axis=1)
    slots = flat * capacity + ranks
    source = jnp.full((fs_count * capacity,), count, jnp.int32)
    source = source.at[slots].set(jnp.arange(count, dtype=jnp.int32))
    filled = (source < count)[:, None]
    row_of = jnp.minimum(source // top, tok_rows - 1)
    whole = lax.all_gather(tokens, "tp", axis=1, tiled=True)
    normed = normalize(whole)
    packed = jnp.where(filled, normed[row_of], jnp.zeros((), jnp.bfloat16))
    arrived = lax.all_to_all(
        packed.reshape(fs_count, capacity, -1), "fs", split_axis=0, concat_axis=0, tiled=True
    )
    arrived = arrived.reshape(fs_count * capacity, -1)
    gate_act = jnp.dot(arrived, gate_out[0], preferred_element_type=jnp.float32)
    up_act = jnp.dot(arrived, up_out[0], preferred_element_type=jnp.float32)
    hidden = (jax.nn.silu(gate_act) * up_act).astype(jnp.bfloat16)
    slot_rows = hidden.shape[0]
    unit_rows = down_out.shape[1]
    hidden_all = lax.all_gather(hidden, "tp", axis=1, tiled=True)
    column_block = lax.all_to_all(
        down_out[0].reshape(unit_rows, tp_count, -1), "tp", split_axis=1, concat_axis=0, tiled=True
    )
    column_block = column_block.reshape(tp_count, unit_rows, -1)
    hidden_blocks = hidden_all.reshape(slot_rows, tp_count, unit_rows)
    partial_value = jnp.einsum(
        "sju,jud->sjd", hidden_blocks, column_block, preferred_element_type=jnp.float32
    ).astype(jnp.bfloat16)
    expert_out = jnp.sum(partial_value, axis=1, dtype=jnp.float32).astype(jnp.bfloat16)
    returned = lax.all_to_all(
        expert_out.reshape(fs_count, capacity, -1), "fs", split_axis=0, concat_axis=0, tiled=True
    )
    returned = returned.reshape(fs_count * capacity, -1)
    picked = returned[slots].reshape(tok_rows, top, -1)
    share = route_weight / jnp.sum(route_weight, axis=1, keepdims=True)
    mixed = jnp.sum(share[:, :, None] * picked.astype(jnp.float32), axis=1).astype(jnp.bfloat16)
    return (gate_out, up_out, down_out, mixed)


MESH = pl.DeviceIdType.MESH
VMEM_BYTES = 67043328


def flip(index, mask):
    other = index
    bit = 1
    while bit <= mask:
        if mask & bit:
            other = other + (1 - 2 * lax.rem(lax.div(index, bit), 2)) * bit
        bit *= 2
    return other


def serve_kernel(
    fs, tp, cap,
    routes_ref, rw_ref, gain_ref, tokens_hbm, gw_hbm, uw_hbm, dw_hbm,
    gat, upw, dn, r, picks_ref, share_ref,
    tokens_ref, gw, uw, dw, gsend, usend, dsend,
    psend, fsend, ftoks, rsend, froutes, x, n, h, wd, y,
    load_sem,
    w_s, w_r, t_s, t_r, p_s, p_r, xf_s, xf_r, h_s, h_r, wd_s, wd_r, y_s, y_r, own_sem,
):
    me = lax.axis_index("fs")
    mt = lax.axis_index("tp")
    toks, cols = tokens_ref.shape
    rows = gw.shape[1]
    units = gw.shape[2]
    each = cols // rows
    slots = fs * cap
    half = fs // 2
    side = lax.div(me, half)
    across = flip(me, half)
    outer = (me < fs // 4) | (me >= fs - fs // 4)
    near = list(range(half - 1, 0, -1))
    far = list(range(fs - 1, half - 1, -1))
    order = [i for pair in zip(far, near + [0]) for i in pair if i]
    direct = [1] + list(range(2, tp, 2))
    relayed = list(range(2, tp, 2))

    loads = [
        pltpu.make_async_copy(src, dst, load_sem.at[k])
        for k, (src, dst) in enumerate(
            ((gw_hbm, gw), (uw_hbm, uw), (dw_hbm, dw), (tokens_hbm, tokens_ref))
        )
    ]
    for load in loads[3:] + loads[:3]:
        load.start()

    barrier = pltpu.get_barrier_semaphore()
    for i in range(fs):
        for j in range(tp):
            if (i == 0) != (j == 0):
                pl.semaphore_signal(
                    barrier, inc=1, device_id=(flip(me, i), flip(mt, j)), device_id_type=MESH
                )

    def remote(src, dst, s, d, device):
        return pltpu.make_async_remote_copy(
            src_ref=src, dst_ref=dst, send_sem=s, recv_sem=d, device_id=device, device_id_type=MESH
        )

    def drain(ref, sem):
        pltpu.make_async_copy(ref, ref, sem).wait()

    def send(*args):
        copy = remote(*args)
        copy.start()
        return copy

    earlier = lax.broadcasted_iota(jnp.int32, (toks, toks), 0) < lax.broadcasted_iota(
        jnp.int32, (toks, toks), 1
    )
    earlier = jnp.where(earlier, 1.0, 0.0).astype(jnp.bfloat16)
    place = lax.broadcasted_iota(jnp.int32, (cap, toks), 0).astype(jnp.float32)

    def ranks(one, two, lowest):
        expert = lax.broadcasted_iota(jnp.int32, (fs, toks), 0) + lowest
        member = (expert == one) | (expert == two)
        rank = jnp.dot(
            jnp.where(member, 1.0, 0.0).astype(jnp.bfloat16), earlier,
            preferred_element_type=jnp.float32,
        )
        return jnp.where(member, rank, -1.0)

    def pack(rank, rows_of, into):
        for e in range(half):
            hit = jnp.where(place == rank[e:e + 1, :], 1.0, 0.0).astype(jnp.bfloat16)
            into[e] = jnp.dot(hit, rows_of, preferred_element_type=jnp.float32).astype(jnp.bfloat16)

    first, second = routes_ref[0:1, :], routes_ref[1:2, :]
    rsend[0:2, :] = routes_ref[...]
    rank = ranks(first, second, side * half)
    loads[3].wait()
    pack(rank, tokens_ref[...], psend)
    x[mt, me] = psend[lax.rem(me, half)]

    pl.semaphore_wait(barrier, fs - 1 + tp - 1)

    crossing = [
        send(rsend, froutes, t_s.at[0], t_r.at[0], (across, mt)),
        send(tokens_ref, ftoks, t_s.at[1], t_r.at[1], (across, mt)),
    ]
    spread = {}

    def dispatch(buf, block, base):
        for i in near:
            peer = flip(me, i)
            spread[base + i] = send(
                buf.at[lax.rem(peer, half)], x.at[mt, block], p_s.at[0], p_r.at[base + i],
                (peer, mt),
            )

    def forward(i):
        block = flip(me, i)
        for j in direct:
            send(
                x.at[mt, block], x.at[mt, block], xf_s.at[0], xf_r.at[j, i // half], (me, flip(mt, j))
            )

    dispatch(psend, me, 0)
    forward(0)

    gain = jnp.broadcast_to(gain_ref[...], (units, rows)).T
    placed = {}
    owns = []
    held = {}
    for k, (raw, buf, dst) in enumerate(((gw, gsend, gat), (uw, usend, upw), (dw, dsend, dn))):
        loads[k].wait()
        for e in range(fs):
            buf[e] = (gain * raw[e] if k < 2 else raw[e]).astype(jnp.bfloat16)
        target = dst.at[me] if k < 2 else dst.at[:, pl.ds(pl.multiple_of(me * rows, rows), rows)]
        held[k] = []
        for i in order:
            peer = flip(me, i)
            arrived = (0 if k == 0 else near[0] if k == 2 and i < half else i)
            copy = remote(buf.at[peer], target, w_s.at[k], w_r.at[k, arrived], (peer, mt))
            placed[k, i] = copy
            if i >= half:
                pl.when(jnp.logical_not(outer))(copy.start)
                held[k].append(copy)
        own = pltpu.make_async_copy(buf.at[me], target, own_sem.at[k])
        own.start()
        owns.append(own)

    def release(k):
        def start():
            for copy in held[k]:
                copy.start()
        pl.when(outer)(start)

    for copy in crossing:
        copy.wait_recv()
    pack(ranks(froutes[0:1, :], froutes[1:2, :], side * half), ftoks[...], fsend)
    x[mt, across] = fsend[lax.rem(me, half)]
    dispatch(fsend, across, half)
    forward(half)
    for k in range(3):
        for i in near:
            placed[k, i].start()
    release(0)
    release(1)
    for i in near:
        spread[i].wait_recv()
        forward(i)
    for i in near:
        spread[half + i].wait_recv()
        forward(half + i)

    for v in range(2):
        first_block = pl.multiple_of((1 - side if v else side) * half, half)
        for j in relayed:
            landed = x.at[flip(mt, j), pl.ds(first_block, half)]
            drain(landed, xf_r.at[j, v])
            send(landed, landed, xf_s.at[0], xf_r.at[j + 1, v], (me, flip(mt, 1)))

    def gather(masks):
        for i in masks:
            if i == 0:
                owns[2].wait()
            elif i >= half:
                placed[2, i].wait_recv()
            elif i == near[0]:
                drain(dsend.at[pl.ds(0, half - 1)], w_r.at[2, i])
            piece = flip(me, i)
            owner, part = lax.rem(piece, tp), lax.div(piece, tp)
            block = dn.at[:, pl.ds(pl.multiple_of(piece * rows, rows), rows)]
            landing = wd_r.at[i // half]
            stays = pltpu.make_async_copy(block, wd.at[mt, part], landing)
            goes = remote(block, wd.at[mt, part], wd_s.at[0], landing, (me, owner))
            pl.when(owner == mt)(stays.start)
            pl.when(owner != mt)(goes.start)

    rank = ranks(first, second, 0)
    hits = [jnp.where(place == rank[e:e + 1, :], 1.0, 0.0) for e in range(fs)]
    gather([0] + near)
    for k, named in enumerate((first, second)):
        picked = jnp.concatenate([jnp.where(named == e, hits[e], 0.0) for e in range(fs)], axis=0)
        picks_ref[k] = picked.T.astype(jnp.bfloat16)
        weight = rw_ref[k:k + 1, :] / (rw_ref[0:1, :] + rw_ref[1:2, :])
        share_ref[k] = jnp.broadcast_to(weight, (toks, toks)).T

    for v in range(2):
        for j in range(1, tp, 2):
            drain(x.at[0, pl.ds(0, half)], xf_r.at[j, v])

    for s in range(fs):
        total = jnp.zeros((cap, 1), jnp.float32)
        for j in range(tp):
            value = x[j, s].astype(jnp.float32)
            total = total + jnp.sum(value * value, axis=-1, keepdims=True)
        scale = lax.rsqrt(total / (tp * cols) + 1e-06)
        for j in range(tp):
            normed = (x[j, s].astype(jnp.float32) * scale).astype(jnp.bfloat16)
            for part in range(each):
                n[j * each + part, s * cap:(s + 1) * cap] = normed[:, part * rows:(part + 1) * rows]

    def activate(k, dst):
        act = jnp.zeros((slots, units), jnp.float32)
        for i in [0] + order:
            if i == 0:
                owns[k].wait()
            elif k == 1:
                placed[k, i].wait_recv()
            elif i == order[0]:
                drain(dst.at[pl.ds(0, fs - 1)], w_r.at[0, 0])
            piece = flip(me, i)
            act = act + jnp.dot(n[piece], dst[piece], preferred_element_type=jnp.float32)
        return act

    gate_act = activate(0, gat)
    gate_act = gate_act / (1.0 + jnp.exp(-gate_act))
    up_act = activate(1, upw)
    h[mt] = (gate_act * up_act).astype(jnp.bfloat16)
    shared = {j: send(h.at[mt], h.at[mt], h_s.at[0], h_r.at[j], (me, flip(mt, j))) for j in direct}
    release(2)
    for j in relayed:
        shared[j].wait_recv()
        source = flip(mt, j)
        shared[j + 1] = send(
            h.at[source], h.at[source], h_s.at[0], h_r.at[j + 1], (me, flip(mt, 1))
        )

    moves = []

    def give_back(late):
        waiting = []
        first_part = (1 - side if late else side) * (each // 2)
        drain(wd.at[:, pl.ds(0, each // 2)], wd_r.at[late])
        for q in range(each // 2):
            part = first_part + q
            result = jnp.zeros((slots, rows), jnp.float32)
            for j in range(tp):
                term = jnp.dot(h[j], wd[j, part], preferred_element_type=jnp.float32)
                result = result + term.astype(jnp.bfloat16).astype(jnp.float32)
            v = late * (each // 2) + q
            y[v] = result.astype(jnp.bfloat16).reshape(fs, cap, rows)
            piece = part * tp + mt
            home, slot = lax.div(piece, each), lax.rem(piece, each)
            for i in far + near:
                peer = flip(me, i)
                copy = remote(y.at[v, peer], r.at[slot, me], y_s.at[0], y_r.at[0], (peer, home))
                if late or i < half:
                    copy.start()
                else:
                    pl.when(jnp.logical_not(outer))(copy.start)
                    waiting.append(copy)
            stays = pltpu.make_async_copy(y.at[v, me], r.at[slot, me], y_r.at[0])
            goes = remote(y.at[v, me], r.at[slot, me], y_s.at[1 + v], y_r.at[0], (me, home))
            pl.when(home == mt)(stays.start)
            pl.when(home != mt)(goes.start)
            moves.append((home != mt, goes))
        return waiting

    for j, copy in shared.items():
        if j % 2:
            copy.wait_recv()
    held[3] = give_back(0)
    gather(far)
    release(3)
    give_back(1)

    drain(r, y_r.at[0])
    for copy in crossing:
        copy.wait_send()
    for k, buf in enumerate((gsend, usend, dsend)):
        drain(buf.at[pl.ds(0, fs - 1)], w_s.at[k])
    for _ in range(2):
        drain(psend.at[pl.ds(0, half - 1)], p_s.at[0])
    for _ in range(tp - 1):
        drain(x.at[0], xf_s.at[0])
    drain(h.at[pl.ds(0, tp - 1)], h_s.at[0])
    for _ in range(tp - 1):
        drain(wd.at[0], wd_s.at[0])
    drain(y.at[:, pl.ds(0, fs - 1)], y_s.at[0])
    for away, goes in moves:
        pl.when(away)(goes.wait_send)


def mix_kernel(gat, upw, dn, r, picks_ref, share_ref, gate_hbm, up_hbm, down_hbm, mixed_hbm, mixed, sem):
    outs = [
        pltpu.make_async_copy(src, dst, sem.at[k])
        for k, (src, dst) in enumerate(
            ((gat, gate_hbm), (upw, up_hbm), (dn, down_hbm), (mixed, mixed_hbm))
        )
    ]
    for copy in outs[:3]:
        copy.start()
    each, fs, cap, rows = r.shape
    for slot in range(each):
        back = r[slot].reshape(fs * cap, rows)
        total = jnp.zeros((mixed.shape[0], rows), jnp.float32)
        for k in range(2):
            term = jnp.dot(picks_ref[k], back, preferred_element_type=jnp.float32)
            total = total + share_ref[k][:, 0:1] * term
        mixed[:, slot * rows:(slot + 1) * rows] = total.astype(jnp.bfloat16)
    outs[3].start()
    for copy in outs:
        copy.wait()


def fused(tokens, routes, route_weight, gain, gate_weight, up_weight, down_weight):
    fs = lax.axis_size("fs")
    tp = lax.axis_size("tp")
    toks, cols = tokens.shape
    top = routes.shape[1]
    cap = capacity_of(toks, top, fs)
    rows, units = gate_weight.shape[1:]
    each = cols // rows
    slots = fs * cap
    bf, f32 = jnp.bfloat16, jnp.float32
    hbm, vmem = pl.BlockSpec(memory_space=pltpu.HBM), pl.BlockSpec(memory_space=pltpu.VMEM)
    dma = pltpu.SemaphoreType.DMA
    kept = 2 * (3 * fs * rows * units + slots * cols + top * toks * slots) + 4 * top * toks * toks
    landed = pl.pallas_call(
        functools.partial(serve_kernel, fs, tp, cap),
        out_shape=(
            pltpu.VMEM((fs, rows, units), bf),
            pltpu.VMEM((fs, rows, units), bf),
            pltpu.VMEM((units, fs * rows), bf),
            pltpu.VMEM((each, fs, cap, rows), bf),
            pltpu.VMEM((top, toks, slots), bf),
            pltpu.VMEM((top, toks, toks), f32),
        ),
        in_specs=[vmem] * 3 + [hbm] * 4,
        out_specs=(vmem,) * 6,
        scratch_shapes=[
            pltpu.VMEM((toks, cols), bf),
            pltpu.VMEM((fs, rows, units), f32),
            pltpu.VMEM((fs, rows, units), f32),
            pltpu.VMEM((fs, units, rows), f32),
            pltpu.VMEM((fs, rows, units), bf),
            pltpu.VMEM((fs, rows, units), bf),
            pltpu.VMEM((fs, units, rows), bf),
            pltpu.VMEM((fs // 2, cap, cols), bf),
            pltpu.VMEM((fs // 2, cap, cols), bf),
            pltpu.VMEM((toks, cols), bf),
            pltpu.VMEM((8, toks), jnp.int32),
            pltpu.VMEM((8, toks), jnp.int32),
            pltpu.VMEM((tp, fs, cap, cols), bf),
            pltpu.VMEM((fs, slots, rows), bf),
            pltpu.VMEM((tp, slots, units), bf),
            pltpu.VMEM((tp, each, units, rows), bf),
            pltpu.VMEM((each, fs, cap, rows), bf),
            dma((4,)),
            dma((3,)), dma((3, fs)), dma((2,)), dma((2,)), dma((1,)), dma((fs,)),
            dma((1,)), dma((tp, 2)), dma((1,)), dma((tp,)),
            dma((1,)), dma((2,)), dma((1 + each,)), dma((1,)), dma((3,)),
        ],
        compiler_params=pltpu.CompilerParams(
            collective_id=0, has_side_effects=True, vmem_limit_bytes=VMEM_BYTES - kept - 2**16
        ),
        name="serve",
    )(routes.T, route_weight.T, gain.reshape(1, -1), tokens, gate_weight, up_weight, down_weight)
    gate, up, down, mixed = pl.pallas_call(
        mix_kernel,
        out_shape=(
            jax.ShapeDtypeStruct((fs, rows, units), bf),
            jax.ShapeDtypeStruct((fs, rows, units), bf),
            jax.ShapeDtypeStruct((units, fs * rows), bf),
            jax.ShapeDtypeStruct((toks, cols), bf),
        ),
        in_specs=[vmem] * 6,
        out_specs=(hbm,) * 4,
        scratch_shapes=[pltpu.VMEM((toks, cols), bf), dma((4,))],
        compiler_params=pltpu.CompilerParams(vmem_limit_bytes=16 * 2**20),
        name="mix",
    )(*landed)
    return (
        gate.reshape(1, fs * rows, units),
        up.reshape(1, fs * rows, units),
        down[None],
        mixed,
    )


def capacity_of(tok_rows, top, fs_count):
    return min(tok_rows, max(2, 3 * tok_rows * top // (2 * fs_count)))


def one_kernel(fs, tp, toks, top, experts, rows, units, cols):
    cap = capacity_of(toks, top, fs)
    powers = fs & (fs - 1) == 0 and tp & (tp - 1) == 0 and fs >= 4 and tp >= 2
    small = fs <= 16 and tp <= 8 and top == 2 and experts == fs
    tiled = cap % 16 == 0 and rows % 128 == 0 and units % 128 == 0 and toks % 128 == 0
    return powers and small and tiled and cols % (2 * rows) == 0 and fs * rows == tp * cols


def program(*args):
    tokens, routes, gate_weight = args[0], args[1], args[4]
    experts, rows, units = gate_weight.shape
    if one_kernel(
        lax.axis_size("fs"), lax.axis_size("tp"), tokens.shape[0], routes.shape[1],
        experts, rows, units, tokens.shape[1],
    ):
        return fused(*args)
    return local(*args)


def solution(mesh):
    in_specs = (
        P("fs", "tp"),
        P("fs", None),
        P("fs", None),
        P("fs"),
        P(None, "fs", "tp"),
        P(None, "fs", "tp"),
        P(None, "tp", "fs"),
    )
    out_specs = (P("fs", None, "tp"), P("fs", None, "tp"), P("fs", "tp", None), P("fs", "tp"))
    return jax.shard_map(program, mesh=mesh, in_specs=in_specs, out_specs=out_specs, check_vma=False)
```

```python
import functools

import jax
import jax.numpy as jnp
from jax import lax
from jax.experimental import pallas as pl
from jax.experimental.pallas import tpu as pltpu
from jax.sharding import PartitionSpec as P


def normalize(rows):
    values = rows.astype(jnp.float32)
    return (values * lax.rsqrt(jnp.mean(values * values, axis=-1, keepdims=True) + 1e-06)).astype(
        jnp.bfloat16
    )


def local(tokens, routes, route_weight, gain, gate_weight, up_weight, down_weight):
    fs_count = lax.axis_size("fs")
    tp_count = lax.axis_size("tp")
    gain_rows = gain[None, :, None]
    gate_new = (gain_rows * gate_weight).astype(jnp.bfloat16)
    up_new = (gain_rows * up_weight).astype(jnp.bfloat16)
    gate_out, up_out = (
        lax.all_to_all(gate_new, "fs", split_axis=0, concat_axis=1, tiled=True),
        lax.all_to_all(up_new, "fs", split_axis=0, concat_axis=1, tiled=True),
    )
    down_out = lax.all_to_all(
        down_weight.astype(jnp.bfloat16), "fs", split_axis=0, concat_axis=2, tiled=True
    )
    tok_rows, top = routes.shape
    capacity = min(tok_rows, max(2, 3 * tok_rows * top // (2 * fs_count)))
    flat = routes.reshape(-1)
    count = flat.shape[0]
    hits = (flat[:, None] == jnp.arange(fs_count, dtype=jnp.int32)[None, :]).astype(jnp.int32)
    ranks = jnp.sum((jnp.cumsum(hits, axis=0) - 1) * hits, axis=1)
    slots = flat * capacity + ranks
    source = jnp.full((fs_count * capacity,), count, jnp.int32)
    source = source.at[slots].set(jnp.arange(count, dtype=jnp.int32))
    filled = (source < count)[:, None]
    row_of = jnp.minimum(source // top, tok_rows - 1)
    whole = lax.all_gather(tokens, "tp", axis=1, tiled=True)
    normed = normalize(whole)
    packed = jnp.where(filled, normed[row_of], jnp.zeros((), jnp.bfloat16))
    arrived = lax.all_to_all(
        packed.reshape(fs_count, capacity, -1), "fs", split_axis=0, concat_axis=0, tiled=True
    )
    arrived = arrived.reshape(fs_count * capacity, -1)
    gate_act = jnp.dot(arrived, gate_out[0], preferred_element_type=jnp.float32)
    up_act = jnp.dot(arrived, up_out[0], preferred_element_type=jnp.float32)
    hidden = (jax.nn.silu(gate_act) * up_act).astype(jnp.bfloat16)
    slot_rows = hidden.shape[0]
    unit_rows = down_out.shape[1]
    hidden_all = lax.all_gather(hidden, "tp", axis=1, tiled=True)
    column_block = lax.all_to_all(
        down_out[0].reshape(unit_rows, tp_count, -1), "tp", split_axis=1, concat_axis=0, tiled=True
    )
    column_block = column_block.reshape(tp_count, unit_rows, -1)
    hidden_blocks = hidden_all.reshape(slot_rows, tp_count, unit_rows)
    partial_value = jnp.einsum(
        "sju,jud->sjd", hidden_blocks, column_block, preferred_element_type=jnp.float32
    ).astype(jnp.bfloat16)
    expert_out = jnp.sum(partial_value, axis=1, dtype=jnp.float32).astype(jnp.bfloat16)
    returned = lax.all_to_all(
        expert_out.reshape(fs_count, capacity, -1), "fs", split_axis=0, concat_axis=0, tiled=True
    )
    returned = returned.reshape(fs_count * capacity, -1)
    picked = returned[slots].reshape(tok_rows, top, -1)
    share = route_weight / jnp.sum(route_weight, axis=1, keepdims=True)
    mixed = jnp.sum(share[:, :, None] * picked.astype(jnp.float32), axis=1).astype(jnp.bfloat16)
    return (gate_out, up_out, down_out, mixed)


MESH = pl.DeviceIdType.MESH
VMEM_BYTES = 67043328


def flip(index, mask):
    other = index
    bit = 1
    while bit <= mask:
        if mask & bit:
            other = other + (1 - 2 * lax.rem(lax.div(index, bit), 2)) * bit
        bit *= 2
    return other


def serve_kernel(
    fs, tp, cap,
    routes_ref, rw_ref, gain_ref, tokens_hbm, gw_hbm, uw_hbm, dw_hbm,
    gat, upw, dn, r, picks_ref, share_ref,
    tokens_ref, gw, uw, dw, gsend, usend, dsend,
    psend, fsend, ftoks, rsend, froutes, x, n, h, wd, y,
    load_sem,
    w_s, w_r, t_s, t_r, p_s, p_r, xf_s, xf_r, h_s, h_r, wd_s, wd_r, y_s, y_r, own_sem, met,
):
    me = lax.axis_index("fs")
    mt = lax.axis_index("tp")
    toks, cols = tokens_ref.shape
    rows = gw.shape[1]
    units = gw.shape[2]
    each = cols // rows
    slots = fs * cap
    half = fs // 2
    side = lax.div(me, half)
    bridge = half | half // 2
    across = flip(me, bridge)
    outer = (me < fs // 4) | (me >= fs - fs // 4)
    near = list(range(half - 1, 0, -1))
    far = [flip(me, i) for i in range(fs - 1, half - 1, -1)]
    homeward = [jnp.where(side == 1, q, fs - 1 - q) for q in range(half)]
    links = [(i, 0) for i in [1 << b for b in range(half.bit_length() - 1)] + [bridge]]
    links += [(0, 1 << b) for b in range(tp.bit_length() - 1)]
    direct = [1] + list(range(2, tp, 2))
    relayed = list(range(2, tp, 2))

    loads = [
        pltpu.make_async_copy(src, dst, load_sem.at[k])
        for k, (src, dst) in enumerate(
            ((gw_hbm, gw), (uw_hbm, uw), (dw_hbm, dw), (tokens_hbm, tokens_ref))
        )
    ]
    for load in loads[3:] + loads[:3]:
        load.start()

    barrier = pltpu.get_barrier_semaphore()

    def greet(sem):
        for i, j in links:
            pl.semaphore_signal(
                sem, inc=1, device_id=(flip(me, i), flip(mt, j)), device_id_type=MESH
            )

    greet(barrier)

    def remote(src, dst, s, d, device):
        return pltpu.make_async_remote_copy(
            src_ref=src, dst_ref=dst, send_sem=s, recv_sem=d, device_id=device, device_id_type=MESH
        )

    def drain(ref, sem):
        pltpu.make_async_copy(ref, ref, sem).wait()

    def send(*args):
        copy = remote(*args)
        copy.start()
        return copy

    earlier = lax.broadcasted_iota(jnp.int32, (toks, toks), 0) < lax.broadcasted_iota(
        jnp.int32, (toks, toks), 1
    )
    earlier = jnp.where(earlier, 1.0, 0.0).astype(jnp.bfloat16)
    place = lax.broadcasted_iota(jnp.int32, (cap, toks), 0).astype(jnp.float32)

    def ranks(one, two, lowest):
        expert = lax.broadcasted_iota(jnp.int32, (fs, toks), 0) + lowest
        member = (expert == one) | (expert == two)
        rank = jnp.dot(
            jnp.where(member, 1.0, 0.0).astype(jnp.bfloat16), earlier,
            preferred_element_type=jnp.float32,
        )
        return jnp.where(member, rank, -1.0)

    def pack(rank, rows_of, into):
        for e in range(half):
            hit = jnp.where(place == rank[e:e + 1, :], 1.0, 0.0).astype(jnp.bfloat16)
            into[e] = jnp.dot(hit, rows_of, preferred_element_type=jnp.float32).astype(jnp.bfloat16)

    first, second = routes_ref[0:1, :], routes_ref[1:2, :]
    rsend[0:2, :] = routes_ref[...]
    rank = ranks(first, second, side * half)
    loads[3].wait()
    pack(rank, tokens_ref[...], psend)
    x[mt, me] = psend[lax.rem(me, half)]

    pl.semaphore_wait(barrier, len(links))
    greet(met.at[0])
    crossing = [
        send(rsend, froutes, t_s.at[0], t_r.at[0], (across, mt)),
        send(tokens_ref, ftoks, t_s.at[1], t_r.at[1], (across, mt)),
    ]
    pl.semaphore_wait(met.at[0], len(links))
    greet(met.at[1])
    pl.semaphore_wait(met.at[1], len(links))

    spread = {}

    def dispatch(buf, block, base):
        for i in near:
            peer = flip(me, i)
            spread[base + i] = send(
                buf.at[lax.rem(peer, half)], x.at[mt, block], p_s.at[0], p_r.at[base + i],
                (peer, mt),
            )

    def forward(i, apart):
        block = flip(me, i ^ bridge if apart else i)
        for j in direct:
            send(
                x.at[mt, block], x.at[mt, block], xf_s.at[0], xf_r.at[j, apart], (me, flip(mt, j))
            )

    dispatch(psend, me, 0)
    forward(0, 0)

    gain = jnp.broadcast_to(gain_ref[...], (units, rows)).T
    placed = {}
    owns = []
    held = {}
    for k, (raw, buf, dst) in enumerate(((gw, gsend, gat), (uw, usend, upw), (dw, dsend, dn))):
        loads[k].wait()
        for e in range(fs):
            buf[e] = (gain * raw[e] if k < 2 else raw[e]).astype(jnp.bfloat16)
        target = dst.at[me] if k < 2 else dst.at[:, pl.ds(pl.multiple_of(me * rows, rows), rows)]
        held[k] = []
        base = 0 if k == 0 else 2 if k == 1 else 3 + half
        for i in near:
            peer = flip(me, i)
            placed[k, i] = remote(buf.at[peer], target, w_s.at[k], w_r.at[base], (peer, mt))
            if k == 0:
                placed[k, i].start()
        for v, peer in enumerate(far):
            arrived = base + 1 + (v if k else 0)
            copy = remote(buf.at[peer], target, w_s.at[k], w_r.at[arrived], (peer, mt))
            pl.when(jnp.logical_not(outer))(copy.start)
            held[k].append((outer, copy))
        own = pltpu.make_async_copy(buf.at[me], target, own_sem.at[k])
        own.start()
        owns.append(own)

    def release(k):
        for when, copy in held[k]:
            pl.when(when)(copy.start)

    for copy in crossing:
        copy.wait_recv()
    pack(ranks(froutes[0:1, :], froutes[1:2, :], side * half), ftoks[...], fsend)
    x[mt, across] = fsend[lax.rem(me, half)]
    dispatch(fsend, across, half)
    forward(0, 1)
    for k in (1, 2):
        for i in near:
            placed[k, i].start()
    release(0)
    release(1)
    for i in near:
        spread[i].wait_recv()
        forward(i, 0)
    for i in near:
        spread[half + i].wait_recv()
        forward(i, 1)

    for v in range(2):
        first_block = pl.multiple_of((1 - side if v else side) * half, half)
        for j in relayed:
            landed = x.at[flip(mt, j), pl.ds(first_block, half)]
            drain(landed, xf_r.at[j, v])
            send(landed, landed, xf_s.at[0], xf_r.at[j + 1, v], (me, flip(mt, 1)))

    def gather(apart):
        for v in range(half):
            if apart:
                drain(dsend.at[0], w_r.at[4 + half + v])
            elif v == 0:
                owns[2].wait()
                drain(dsend.at[pl.ds(0, half - 1)], w_r.at[3 + half])
            piece = far[v] if apart else flip(me, v)
            owner, part = lax.rem(piece, tp), lax.div(piece, tp)
            block = dn.at[:, pl.ds(pl.multiple_of(piece * rows, rows), rows)]
            landing = wd_r.at[apart]
            stays = pltpu.make_async_copy(block, wd.at[mt, part], landing)
            goes = remote(block, wd.at[mt, part], wd_s.at[0], landing, (me, owner))
            pl.when(owner == mt)(stays.start)
            pl.when(owner != mt)(goes.start)

    rank = ranks(first, second, 0)
    hits = [jnp.where(place == rank[e:e + 1, :], 1.0, 0.0) for e in range(fs)]
    for k, named in enumerate((first, second)):
        picked = jnp.concatenate([jnp.where(named == e, hits[e], 0.0) for e in range(fs)], axis=0)
        picks_ref[k] = picked.T.astype(jnp.bfloat16)
        weight = rw_ref[k:k + 1, :] / (rw_ref[0:1, :] + rw_ref[1:2, :])
        share_ref[k] = jnp.broadcast_to(weight, (toks, toks)).T

    for v in range(2):
        for j in range(1, tp, 2):
            drain(x.at[0, pl.ds(0, half)], xf_r.at[j, v])

    for s in range(fs):
        total = jnp.zeros((cap, 1), jnp.float32)
        for j in range(tp):
            value = x[j, s].astype(jnp.float32)
            total = total + jnp.sum(value * value, axis=-1, keepdims=True)
        scale = lax.rsqrt(total / (tp * cols) + 1e-06)
        for j in range(tp):
            normed = (x[j, s].astype(jnp.float32) * scale).astype(jnp.bfloat16)
            for part in range(each):
                n[j * each + part, s * cap:(s + 1) * cap] = normed[:, part * rows:(part + 1) * rows]

    def activate(k, dst):
        base = 0 if k == 0 else 2
        owns[k].wait()
        drain(dst.at[pl.ds(0, half - 1)], w_r.at[base])
        pieces = [me] + [flip(me, i) for i in near] + far
        act = jnp.zeros((slots, units), jnp.float32)
        for v, piece in enumerate(pieces):
            if k == 0 and v == half:
                drain(dst.at[pl.ds(0, half)], w_r.at[base + 1])
            if k == 1 and v >= half:
                drain(dst.at[0], w_r.at[base + 1 + v - half])
            act = act + jnp.dot(n[piece], dst[piece], preferred_element_type=jnp.float32)
        return act

    gate_act = activate(0, gat)
    gate_act = gate_act / (1.0 + jnp.exp(-gate_act))
    gather(0)
    up_act = activate(1, upw)
    h[mt] = (gate_act * up_act).astype(jnp.bfloat16)
    shared = {j: send(h.at[mt], h.at[mt], h_s.at[0], h_r.at[j], (me, flip(mt, j))) for j in direct}
    release(2)
    for j in relayed:
        shared[j].wait_recv()
        source = flip(mt, j)
        shared[j + 1] = send(
            h.at[source], h.at[source], h_s.at[0], h_r.at[j + 1], (me, flip(mt, 1))
        )

    moves = []

    def give_back(late):
        waiting = []
        first_part = (1 - side if late else side) * (each // 2)
        drain(wd.at[:, pl.ds(0, each // 2)], wd_r.at[late])
        for q in range(each // 2):
            part = first_part + q
            result = jnp.zeros((slots, rows), jnp.float32)
            for j in range(tp):
                term = jnp.dot(h[j], wd[j, part], preferred_element_type=jnp.float32)
                result = result + term.astype(jnp.bfloat16).astype(jnp.float32)
            v = late * (each // 2) + q
            y[v] = result.astype(jnp.bfloat16).reshape(fs, cap, rows)
            piece = part * tp + mt
            home, slot = lax.div(piece, each), lax.rem(piece, each)
            for peer in homeward:
                copy = remote(y.at[v, peer], r.at[slot, me], y_s.at[0], y_r.at[0], (peer, home))
                if late:
                    copy.start()
                else:
                    pl.when(jnp.logical_not(outer))(copy.start)
                    waiting.append((outer, copy))
            for i in near:
                peer = flip(me, i)
                send(y.at[v, peer], r.at[slot, me], y_s.at[0], y_r.at[0], (peer, home))
            stays = pltpu.make_async_copy(y.at[v, me], r.at[slot, me], y_r.at[0])
            goes = remote(y.at[v, me], r.at[slot, me], y_s.at[1 + v], y_r.at[0], (me, home))
            pl.when(home == mt)(stays.start)
            pl.when(home != mt)(goes.start)
            moves.append((home != mt, goes))
        return waiting

    for j, copy in shared.items():
        if j % 2:
            copy.wait_recv()
    held[3] = give_back(0)
    gather(1)
    release(3)
    give_back(1)

    drain(r, y_r.at[0])
    for copy in crossing:
        copy.wait_send()
    for k, buf in enumerate((gsend, usend, dsend)):
        drain(buf.at[pl.ds(0, fs - 1)], w_s.at[k])
    for _ in range(2):
        drain(psend.at[pl.ds(0, half - 1)], p_s.at[0])
    for _ in range(tp - 1):
        drain(x.at[0], xf_s.at[0])
    drain(h.at[pl.ds(0, tp - 1)], h_s.at[0])
    for _ in range(tp - 1):
        drain(wd.at[0], wd_s.at[0])
    drain(y.at[:, pl.ds(0, fs - 1)], y_s.at[0])
    for away, goes in moves:
        pl.when(away)(goes.wait_send)


def mix_kernel(gat, upw, dn, r, picks_ref, share_ref, gate_hbm, up_hbm, down_hbm, mixed_hbm, mixed, sem):
    outs = [
        pltpu.make_async_copy(src, dst, sem.at[k])
        for k, (src, dst) in enumerate(
            ((gat, gate_hbm), (upw, up_hbm), (dn, down_hbm), (mixed, mixed_hbm))
        )
    ]
    for copy in outs[:3]:
        copy.start()
    each, fs, cap, rows = r.shape
    for slot in range(each):
        back = r[slot].reshape(fs * cap, rows)
        total = jnp.zeros((mixed.shape[0], rows), jnp.float32)
        for k in range(2):
            term = jnp.dot(picks_ref[k], back, preferred_element_type=jnp.float32)
            total = total + share_ref[k][:, 0:1] * term
        mixed[:, slot * rows:(slot + 1) * rows] = total.astype(jnp.bfloat16)
    outs[3].start()
    for copy in outs:
        copy.wait()


def fused(tokens, routes, route_weight, gain, gate_weight, up_weight, down_weight):
    fs = lax.axis_size("fs")
    tp = lax.axis_size("tp")
    toks, cols = tokens.shape
    top = routes.shape[1]
    cap = capacity_of(toks, top, fs)
    rows, units = gate_weight.shape[1:]
    each = cols // rows
    slots = fs * cap
    bf, f32 = jnp.bfloat16, jnp.float32
    hbm, vmem = pl.BlockSpec(memory_space=pltpu.HBM), pl.BlockSpec(memory_space=pltpu.VMEM)
    dma = pltpu.SemaphoreType.DMA
    kept = 2 * (3 * fs * rows * units + slots * cols + top * toks * slots) + 4 * top * toks * toks
    landed = pl.pallas_call(
        functools.partial(serve_kernel, fs, tp, cap),
        out_shape=(
            pltpu.VMEM((fs, rows, units), bf),
            pltpu.VMEM((fs, rows, units), bf),
            pltpu.VMEM((units, fs * rows), bf),
            pltpu.VMEM((each, fs, cap, rows), bf),
            pltpu.VMEM((top, toks, slots), bf),
            pltpu.VMEM((top, toks, toks), f32),
        ),
        in_specs=[vmem] * 3 + [hbm] * 4,
        out_specs=(vmem,) * 6,
        scratch_shapes=[
            pltpu.VMEM((toks, cols), bf),
            pltpu.VMEM((fs, rows, units), f32),
            pltpu.VMEM((fs, rows, units), f32),
            pltpu.VMEM((fs, units, rows), f32),
            pltpu.VMEM((fs, rows, units), bf),
            pltpu.VMEM((fs, rows, units), bf),
            pltpu.VMEM((fs, units, rows), bf),
            pltpu.VMEM((fs // 2, cap, cols), bf),
            pltpu.VMEM((fs // 2, cap, cols), bf),
            pltpu.VMEM((toks, cols), bf),
            pltpu.VMEM((8, toks), jnp.int32),
            pltpu.VMEM((8, toks), jnp.int32),
            pltpu.VMEM((tp, fs, cap, cols), bf),
            pltpu.VMEM((fs, slots, rows), bf),
            pltpu.VMEM((tp, slots, units), bf),
            pltpu.VMEM((tp, each, units, rows), bf),
            pltpu.VMEM((each, fs, cap, rows), bf),
            dma((4,)),
            dma((3,)), dma((fs + 4,)), dma((2,)), dma((2,)), dma((1,)), dma((fs,)),
            dma((1,)), dma((tp, 2)), dma((1,)), dma((tp,)),
            dma((1,)), dma((2,)), dma((1 + each,)), dma((1,)), dma((3,)),
            pltpu.SemaphoreType.REGULAR((2,)),
        ],
        compiler_params=pltpu.CompilerParams(
            collective_id=0, has_side_effects=True, vmem_limit_bytes=VMEM_BYTES - kept - 2**16
        ),
        name="serve",
    )(routes.T, route_weight.T, gain.reshape(1, -1), tokens, gate_weight, up_weight, down_weight)
    gate, up, down, mixed = pl.pallas_call(
        mix_kernel,
        out_shape=(
            jax.ShapeDtypeStruct((fs, rows, units), bf),
            jax.ShapeDtypeStruct((fs, rows, units), bf),
            jax.ShapeDtypeStruct((units, fs * rows), bf),
            jax.ShapeDtypeStruct((toks, cols), bf),
        ),
        in_specs=[vmem] * 6,
        out_specs=(hbm,) * 4,
        scratch_shapes=[pltpu.VMEM((toks, cols), bf), dma((4,))],
        compiler_params=pltpu.CompilerParams(vmem_limit_bytes=16 * 2**20),
        name="mix",
    )(*landed)
    return (
        gate.reshape(1, fs * rows, units),
        up.reshape(1, fs * rows, units),
        down[None],
        mixed,
    )


def capacity_of(tok_rows, top, fs_count):
    return min(tok_rows, max(2, 3 * tok_rows * top // (2 * fs_count)))


def one_kernel(fs, tp, toks, top, experts, rows, units, cols):
    cap = capacity_of(toks, top, fs)
    powers = fs & (fs - 1) == 0 and tp & (tp - 1) == 0 and fs >= 4 and tp >= 2
    small = fs <= 16 and tp <= 8 and top == 2 and experts == fs
    tiled = cap % 16 == 0 and rows % 128 == 0 and units % 128 == 0 and toks % 128 == 0
    return powers and small and tiled and cols % (2 * rows) == 0 and fs * rows == tp * cols


def program(*args):
    tokens, routes, gate_weight = args[0], args[1], args[4]
    experts, rows, units = gate_weight.shape
    if one_kernel(
        lax.axis_size("fs"), lax.axis_size("tp"), tokens.shape[0], routes.shape[1],
        experts, rows, units, tokens.shape[1],
    ):
        return fused(*args)
    return local(*args)


def solution(mesh):
    in_specs = (
        P("fs", "tp"),
        P("fs", None),
        P("fs", None),
        P("fs"),
        P(None, "fs", "tp"),
        P(None, "fs", "tp"),
        P(None, "tp", "fs"),
    )
    out_specs = (P("fs", None, "tp"), P("fs", None, "tp"), P("fs", "tp", None), P("fs", "tp"))
    return jax.shard_map(program, mesh=mesh, in_specs=in_specs, out_specs=out_specs, check_vma=False)
```

```python
import functools

import jax
import jax.numpy as jnp
from jax import lax
from jax.experimental import pallas as pl
from jax.experimental.pallas import tpu as pltpu
from jax.sharding import PartitionSpec as P


def normalize(rows):
    values = rows.astype(jnp.float32)
    return (values * lax.rsqrt(jnp.mean(values * values, axis=-1, keepdims=True) + 1e-06)).astype(
        jnp.bfloat16
    )


def local(tokens, routes, route_weight, gain, gate_weight, up_weight, down_weight):
    fs_count = lax.axis_size("fs")
    tp_count = lax.axis_size("tp")
    gain_rows = gain[None, :, None]
    gate_new = (gain_rows * gate_weight).astype(jnp.bfloat16)
    up_new = (gain_rows * up_weight).astype(jnp.bfloat16)
    gate_out, up_out = (
        lax.all_to_all(gate_new, "fs", split_axis=0, concat_axis=1, tiled=True),
        lax.all_to_all(up_new, "fs", split_axis=0, concat_axis=1, tiled=True),
    )
    down_out = lax.all_to_all(
        down_weight.astype(jnp.bfloat16), "fs", split_axis=0, concat_axis=2, tiled=True
    )
    tok_rows, top = routes.shape
    capacity = min(tok_rows, max(2, 3 * tok_rows * top // (2 * fs_count)))
    flat = routes.reshape(-1)
    count = flat.shape[0]
    hits = (flat[:, None] == jnp.arange(fs_count, dtype=jnp.int32)[None, :]).astype(jnp.int32)
    ranks = jnp.sum((jnp.cumsum(hits, axis=0) - 1) * hits, axis=1)
    slots = flat * capacity + ranks
    source = jnp.full((fs_count * capacity,), count, jnp.int32)
    source = source.at[slots].set(jnp.arange(count, dtype=jnp.int32))
    filled = (source < count)[:, None]
    row_of = jnp.minimum(source // top, tok_rows - 1)
    whole = lax.all_gather(tokens, "tp", axis=1, tiled=True)
    normed = normalize(whole)
    packed = jnp.where(filled, normed[row_of], jnp.zeros((), jnp.bfloat16))
    arrived = lax.all_to_all(
        packed.reshape(fs_count, capacity, -1), "fs", split_axis=0, concat_axis=0, tiled=True
    )
    arrived = arrived.reshape(fs_count * capacity, -1)
    gate_act = jnp.dot(arrived, gate_out[0], preferred_element_type=jnp.float32)
    up_act = jnp.dot(arrived, up_out[0], preferred_element_type=jnp.float32)
    hidden = (jax.nn.silu(gate_act) * up_act).astype(jnp.bfloat16)
    slot_rows = hidden.shape[0]
    unit_rows = down_out.shape[1]
    hidden_all = lax.all_gather(hidden, "tp", axis=1, tiled=True)
    column_block = lax.all_to_all(
        down_out[0].reshape(unit_rows, tp_count, -1), "tp", split_axis=1, concat_axis=0, tiled=True
    )
    column_block = column_block.reshape(tp_count, unit_rows, -1)
    hidden_blocks = hidden_all.reshape(slot_rows, tp_count, unit_rows)
    partial_value = jnp.einsum(
        "sju,jud->sjd", hidden_blocks, column_block, preferred_element_type=jnp.float32
    ).astype(jnp.bfloat16)
    expert_out = jnp.sum(partial_value, axis=1, dtype=jnp.float32).astype(jnp.bfloat16)
    returned = lax.all_to_all(
        expert_out.reshape(fs_count, capacity, -1), "fs", split_axis=0, concat_axis=0, tiled=True
    )
    returned = returned.reshape(fs_count * capacity, -1)
    picked = returned[slots].reshape(tok_rows, top, -1)
    share = route_weight / jnp.sum(route_weight, axis=1, keepdims=True)
    mixed = jnp.sum(share[:, :, None] * picked.astype(jnp.float32), axis=1).astype(jnp.bfloat16)
    return (gate_out, up_out, down_out, mixed)


MESH = pl.DeviceIdType.MESH
VMEM_BYTES = 67043328


def flip(index, mask):
    other = index
    bit = 1
    while bit <= mask:
        if mask & bit:
            other = other + (1 - 2 * lax.rem(lax.div(index, bit), 2)) * bit
        bit *= 2
    return other


def serve_kernel(
    fs, tp, cap,
    routes_ref, rw_ref, gain_ref, tokens_hbm, gw_hbm, uw_hbm, dw_hbm,
    gat, upw, dn, r, picks_ref, share_ref,
    tokens_ref, gw, uw, dw, gsend, usend, dsend,
    psend, fsend, ftoks, rsend, froutes, x, n, h, wd, y,
    load_sem,
    out, w_r, t_r, p_r, xf_r, h_r, wd_r, y_s, y_r, met,
):
    me = lax.axis_index("fs")
    mt = lax.axis_index("tp")
    toks, cols = tokens_ref.shape
    rows = gw.shape[1]
    units = gw.shape[2]
    each = cols // rows
    slots = fs * cap
    half = fs // 2
    side = lax.div(me, half)
    bridge = half | half // 2
    across = flip(me, bridge)
    outer = (me < fs // 4) | (me >= fs - fs // 4)
    near = list(range(half - 1, 0, -1))
    far = [flip(me, i) for i in range(fs - 1, half - 1, -1)]
    homeward = [jnp.where(side == 1, q, fs - 1 - q) for q in range(half)]
    links = [(i, 0) for i in [1 << b for b in range(half.bit_length() - 1)] + [bridge]]
    links += [(0, 1 << b) for b in range(tp.bit_length() - 1)]
    direct = [1] + list(range(2, tp, 2))
    relayed = list(range(2, tp, 2))

    loads = [
        pltpu.make_async_copy(src, dst, load_sem.at[k])
        for k, (src, dst) in enumerate(
            ((gw_hbm, gw), (uw_hbm, uw), (dw_hbm, dw), (tokens_hbm, tokens_ref))
        )
    ]
    for load in loads[3:] + loads[:3]:
        load.start()

    barrier = pltpu.get_barrier_semaphore()

    def greet(sem):
        for i, j in links:
            pl.semaphore_signal(
                sem, inc=1, device_id=(flip(me, i), flip(mt, j)), device_id_type=MESH
            )

    greet(barrier)

    def remote(src, dst, s, d, device):
        return pltpu.make_async_remote_copy(
            src_ref=src, dst_ref=dst, send_sem=s, recv_sem=d, device_id=device, device_id_type=MESH
        )

    def drain(ref, sem):
        pltpu.make_async_copy(ref, ref, sem).wait()

    def send(*args):
        copy = remote(*args)
        copy.start()
        return copy

    earlier = lax.broadcasted_iota(jnp.int32, (toks, toks), 0) < lax.broadcasted_iota(
        jnp.int32, (toks, toks), 1
    )
    earlier = jnp.where(earlier, 1.0, 0.0).astype(jnp.bfloat16)
    place = lax.broadcasted_iota(jnp.int32, (cap, toks), 0).astype(jnp.float32)

    def ranks(one, two, lowest):
        expert = lax.broadcasted_iota(jnp.int32, (fs, toks), 0) + lowest
        member = (expert == one) | (expert == two)
        rank = jnp.dot(
            jnp.where(member, 1.0, 0.0).astype(jnp.bfloat16), earlier,
            preferred_element_type=jnp.float32,
        )
        return jnp.where(member, rank, -1.0)

    def pack(rank, rows_of, into):
        for e in range(half):
            hit = jnp.where(place == rank[e:e + 1, :], 1.0, 0.0).astype(jnp.bfloat16)
            into[e] = jnp.dot(hit, rows_of, preferred_element_type=jnp.float32).astype(jnp.bfloat16)

    first, second = routes_ref[0:1, :], routes_ref[1:2, :]
    rsend[0:2, :] = routes_ref[...]
    rank = ranks(first, second, side * half)
    loads[3].wait()
    pack(rank, tokens_ref[...], psend)
    x[mt, me] = psend[lax.rem(me, half)]

    pl.semaphore_wait(barrier, len(links))
    greet(met.at[0])
    crossing = [
        send(rsend, froutes, out.at[0], t_r.at[0], (across, mt)),
        send(tokens_ref, ftoks, out.at[0], t_r.at[1], (across, mt)),
    ]
    pl.semaphore_wait(met.at[0], len(links))
    greet(met.at[1])
    pl.semaphore_wait(met.at[1], len(links))

    def dispatch(buf, block, base):
        for i in near:
            peer = flip(me, i)
            send(
                buf.at[lax.rem(peer, half)], x.at[mt, block], out.at[0], p_r.at[base],
                (peer, mt),
            )

    def forward(i, apart):
        block = flip(me, i ^ bridge if apart else i)
        for j in direct:
            send(
                x.at[mt, block], x.at[mt, block], out.at[0], xf_r.at[j - 1, apart], (me, flip(mt, j))
            )

    dispatch(psend, me, 0)
    forward(0, 0)

    gain = jnp.broadcast_to(gain_ref[...], (units, rows)).T
    placed = {}
    held = {}
    for k, (raw, buf, dst) in enumerate(((gw, gsend, gat), (uw, usend, upw), (dw, dsend, dn))):
        loads[k].wait()
        for e in range(fs):
            buf[e] = (gain * raw[e] if k < 2 else raw[e]).astype(jnp.bfloat16)
        target = dst.at[me] if k < 2 else dst.at[:, pl.ds(pl.multiple_of(me * rows, rows), rows)]
        held[k] = []
        base = 0 if k == 0 else 2 if k == 1 else 3 + half
        for i in near:
            peer = flip(me, i)
            placed[k, i] = remote(buf.at[peer], target, out.at[0], w_r.at[base], (peer, mt))
            if k == 0:
                placed[k, i].start()
        for v, peer in enumerate(far):
            arrived = base + 1 + (v if k else 0)
            copy = remote(buf.at[peer], target, out.at[0], w_r.at[arrived], (peer, mt))
            pl.when(jnp.logical_not(outer))(copy.start)
            held[k].append((outer, copy))
        if k < 2:
            dst[me] = buf[me]
        else:
            dst[:, pl.ds(pl.multiple_of(me * rows, rows), rows)] = buf[me]

    def release(k):
        for when, copy in held[k]:
            if when is True:
                copy.start()
            else:
                pl.when(when)(copy.start)

    for copy in crossing:
        copy.wait_recv()
    pack(ranks(froutes[0:1, :], froutes[1:2, :], side * half), ftoks[...], fsend)
    x[mt, across] = fsend[lax.rem(me, half)]
    dispatch(fsend, across, 1)
    forward(0, 1)
    for k in (2, 1):
        for i in near:
            placed[k, i].start()
    release(0)
    release(1)
    for apart in range(2):
        drain(psend.at[pl.ds(0, half - 1)], p_r.at[apart])
        for i in near:
            forward(i, apart)

    for v in range(2):
        first_block = pl.multiple_of((1 - side if v else side) * half, half)
        for j in relayed:
            landed = x.at[flip(mt, j), pl.ds(first_block, half)]
            drain(landed, xf_r.at[j - 1, v])
            send(landed, landed, out.at[0], xf_r.at[j, v], (me, flip(mt, 1)))

    def gather(apart):
        for v in range(half):
            if apart:
                drain(dsend.at[0], w_r.at[4 + half + v])
            elif v == 0:
                drain(dsend.at[pl.ds(0, half - 1)], w_r.at[3 + half])
            piece = far[v] if apart else flip(me, v)
            owner, part = lax.rem(piece, tp), lax.div(piece, tp)
            block = dn.at[:, pl.ds(pl.multiple_of(piece * rows, rows), rows)]
            landing = wd_r.at[apart]
            stays = pltpu.make_async_copy(block, wd.at[mt, part], landing)
            goes = remote(block, wd.at[mt, part], out.at[0], landing, (me, owner))
            pl.when(owner == mt)(stays.start)
            pl.when(owner != mt)(goes.start)

    rank = ranks(first, second, 0)
    hits = [jnp.where(place == rank[e:e + 1, :], 1.0, 0.0) for e in range(fs)]
    for k, named in enumerate((first, second)):
        picked = jnp.concatenate([jnp.where(named == e, hits[e], 0.0) for e in range(fs)], axis=0)
        picks_ref[k] = picked.T.astype(jnp.bfloat16)
        weight = rw_ref[k:k + 1, :] / (rw_ref[0:1, :] + rw_ref[1:2, :])
        share_ref[k] = jnp.broadcast_to(weight, (toks, toks)).T

    for v in range(2):
        for j in range(1, tp, 2):
            drain(x.at[0, pl.ds(0, half)], xf_r.at[j - 1, v])

    for s in range(fs):
        total = jnp.zeros((cap, 1), jnp.float32)
        for j in range(tp):
            value = x[j, s].astype(jnp.float32)
            total = total + jnp.sum(value * value, axis=-1, keepdims=True)
        scale = lax.rsqrt(total / (tp * cols) + 1e-06)
        for j in range(tp):
            normed = (x[j, s].astype(jnp.float32) * scale).astype(jnp.bfloat16)
            for part in range(each):
                n[j * each + part, s * cap:(s + 1) * cap] = normed[:, part * rows:(part + 1) * rows]

    def activate(k, dst):
        base = 0 if k == 0 else 2
        drain(dst.at[pl.ds(0, half - 1)], w_r.at[base])
        pieces = [me] + [flip(me, i) for i in near] + far
        act = jnp.zeros((slots, units), jnp.float32)
        for v, piece in enumerate(pieces):
            if k == 0 and v == half:
                drain(dst.at[pl.ds(0, half)], w_r.at[base + 1])
            if k == 1 and v >= half:
                drain(dst.at[0], w_r.at[base + 1 + v - half])
            act = act + jnp.dot(n[piece], dst[piece], preferred_element_type=jnp.float32)
        return act

    gate_act = activate(0, gat)
    gate_act = gate_act / (1.0 + jnp.exp(-gate_act))
    gather(0)
    up_act = activate(1, upw)
    h[mt] = (gate_act * up_act).astype(jnp.bfloat16)
    shared = {j: send(h.at[mt], h.at[mt], out.at[0], h_r.at[j - 1], (me, flip(mt, j))) for j in direct}
    release(2)
    for j in relayed:
        shared[j].wait_recv()
        source = flip(mt, j)
        shared[j + 1] = send(
            h.at[source], h.at[source], out.at[0], h_r.at[j], (me, flip(mt, 1))
        )

    moves = []

    def give_back(late):
        waiting = []
        first_part = (1 - side if late else side) * (each // 2)
        drain(wd.at[:, pl.ds(0, each // 2)], wd_r.at[late])
        for q in range(each // 2):
            part = first_part + q
            result = jnp.zeros((slots, rows), jnp.float32)
            for j in range(tp):
                term = jnp.dot(h[j], wd[j, part], preferred_element_type=jnp.float32)
                result = result + term.astype(jnp.bfloat16).astype(jnp.float32)
            v = late * (each // 2) + q
            y[v] = result.astype(jnp.bfloat16).reshape(fs, cap, rows)
            piece = part * tp + mt
            home, slot = lax.div(piece, each), lax.rem(piece, each)
            for peer in homeward:
                copy = remote(y.at[v, peer], r.at[slot, me], out.at[0], y_r.at[0], (peer, home))
                if late:
                    copy.start()
                else:
                    waiting.append((True, copy))
            for i in near:
                peer = flip(me, i)
                send(y.at[v, peer], r.at[slot, me], out.at[0], y_r.at[0], (peer, home))
            stays = pltpu.make_async_copy(y.at[v, me], r.at[slot, me], y_r.at[0])
            goes = remote(y.at[v, me], r.at[slot, me], y_s.at[v], y_r.at[0], (me, home))
            pl.when(home == mt)(stays.start)
            pl.when(home != mt)(goes.start)
            moves.append((home != mt, goes))
        return waiting

    for j, copy in shared.items():
        if j % 2:
            copy.wait_recv()
    held[3] = give_back(0)
    gather(1)
    release(3)
    give_back(1)

    drain(r, y_r.at[0])
    for copy in crossing:
        copy.wait_send()
    for k, buf in enumerate((gsend, usend, dsend)):
        drain(buf.at[pl.ds(0, fs - 1)], out.at[0])
    for _ in range(2):
        drain(psend.at[pl.ds(0, half - 1)], out.at[0])
    for _ in range(tp - 1):
        drain(x.at[0], out.at[0])
    drain(h.at[pl.ds(0, tp - 1)], out.at[0])
    for _ in range(tp - 1):
        drain(wd.at[0], out.at[0])
    drain(y.at[:, pl.ds(0, fs - 1)], out.at[0])
    for away, goes in moves:
        pl.when(away)(goes.wait_send)


def mix_kernel(gat, upw, dn, r, picks_ref, share_ref, gate_hbm, up_hbm, down_hbm, mixed_hbm, mixed, sem):
    outs = [
        pltpu.make_async_copy(src, dst, sem.at[k])
        for k, (src, dst) in enumerate(
            ((gat, gate_hbm), (upw, up_hbm), (dn, down_hbm), (mixed, mixed_hbm))
        )
    ]
    for copy in outs[:3]:
        copy.start()
    each, fs, cap, rows = r.shape
    for slot in range(each):
        back = r[slot].reshape(fs * cap, rows)
        total = jnp.zeros((mixed.shape[0], rows), jnp.float32)
        for k in range(2):
            term = jnp.dot(picks_ref[k], back, preferred_element_type=jnp.float32)
            total = total + share_ref[k][:, 0:1] * term
        mixed[:, slot * rows:(slot + 1) * rows] = total.astype(jnp.bfloat16)
    outs[3].start()
    for copy in outs:
        copy.wait()


def fused(tokens, routes, route_weight, gain, gate_weight, up_weight, down_weight):
    fs = lax.axis_size("fs")
    tp = lax.axis_size("tp")
    toks, cols = tokens.shape
    top = routes.shape[1]
    cap = capacity_of(toks, top, fs)
    rows, units = gate_weight.shape[1:]
    each = cols // rows
    slots = fs * cap
    bf, f32 = jnp.bfloat16, jnp.float32
    hbm, vmem = pl.BlockSpec(memory_space=pltpu.HBM), pl.BlockSpec(memory_space=pltpu.VMEM)
    dma = pltpu.SemaphoreType.DMA
    kept = 2 * (3 * fs * rows * units + slots * cols + top * toks * slots) + 4 * top * toks * toks
    landed = pl.pallas_call(
        functools.partial(serve_kernel, fs, tp, cap),
        out_shape=(
            pltpu.VMEM((fs, rows, units), bf),
            pltpu.VMEM((fs, rows, units), bf),
            pltpu.VMEM((units, fs * rows), bf),
            pltpu.VMEM((each, fs, cap, rows), bf),
            pltpu.VMEM((top, toks, slots), bf),
            pltpu.VMEM((top, toks, toks), f32),
        ),
        in_specs=[vmem] * 3 + [hbm] * 4,
        out_specs=(vmem,) * 6,
        scratch_shapes=[
            pltpu.VMEM((toks, cols), bf),
            pltpu.VMEM((fs, rows, units), f32),
            pltpu.VMEM((fs, rows, units), f32),
            pltpu.VMEM((fs, units, rows), f32),
            pltpu.VMEM((fs, rows, units), bf),
            pltpu.VMEM((fs, rows, units), bf),
            pltpu.VMEM((fs, units, rows), bf),
            pltpu.VMEM((fs // 2, cap, cols), bf),
            pltpu.VMEM((fs // 2, cap, cols), bf),
            pltpu.VMEM((toks, cols), bf),
            pltpu.VMEM((8, toks), jnp.int32),
            pltpu.VMEM((8, toks), jnp.int32),
            pltpu.VMEM((tp, fs, cap, cols), bf),
            pltpu.VMEM((fs, slots, rows), bf),
            pltpu.VMEM((tp, slots, units), bf),
            pltpu.VMEM((tp, each, units, rows), bf),
            pltpu.VMEM((each, fs, cap, rows), bf),
            dma((4,)),
            dma((1,)), dma((fs + 4,)), dma((2,)), dma((2,)), dma((tp - 1, 2)), dma((tp - 1,)),
            dma((2,)), dma((each,)), dma((1,)),
            pltpu.SemaphoreType.REGULAR((2,)),
        ],
        compiler_params=pltpu.CompilerParams(
            collective_id=0, has_side_effects=True, vmem_limit_bytes=VMEM_BYTES - kept - 2**16
        ),
        name="serve",
    )(routes.T, route_weight.T, gain.reshape(1, -1), tokens, gate_weight, up_weight, down_weight)
    gate, up, down, mixed = pl.pallas_call(
        mix_kernel,
        out_shape=(
            jax.ShapeDtypeStruct((fs, rows, units), bf),
            jax.ShapeDtypeStruct((fs, rows, units), bf),
            jax.ShapeDtypeStruct((units, fs * rows), bf),
            jax.ShapeDtypeStruct((toks, cols), bf),
        ),
        in_specs=[vmem] * 6,
        out_specs=(hbm,) * 4,
        scratch_shapes=[pltpu.VMEM((toks, cols), bf), dma((4,))],
        compiler_params=pltpu.CompilerParams(vmem_limit_bytes=16 * 2**20),
        name="mix",
    )(*landed)
    return (
        gate.reshape(1, fs * rows, units),
        up.reshape(1, fs * rows, units),
        down[None],
        mixed,
    )


def capacity_of(tok_rows, top, fs_count):
    return min(tok_rows, max(2, 3 * tok_rows * top // (2 * fs_count)))


def one_kernel(fs, tp, toks, top, experts, rows, units, cols):
    cap = capacity_of(toks, top, fs)
    powers = fs & (fs - 1) == 0 and tp & (tp - 1) == 0 and fs >= 4 and tp >= 2
    small = fs <= 16 and tp <= 8 and top == 2 and experts == fs
    tiled = cap % 16 == 0 and rows % 128 == 0 and units % 128 == 0 and toks % 128 == 0
    return powers and small and tiled and cols % (2 * rows) == 0 and fs * rows == tp * cols


def program(*args):
    tokens, routes, gate_weight = args[0], args[1], args[4]
    experts, rows, units = gate_weight.shape
    if one_kernel(
        lax.axis_size("fs"), lax.axis_size("tp"), tokens.shape[0], routes.shape[1],
        experts, rows, units, tokens.shape[1],
    ):
        return fused(*args)
    return local(*args)


def solution(mesh):
    in_specs = (
        P("fs", "tp"),
        P("fs", None),
        P("fs", None),
        P("fs"),
        P(None, "fs", "tp"),
        P(None, "fs", "tp"),
        P(None, "tp", "fs"),
    )
    out_specs = (P("fs", None, "tp"), P("fs", None, "tp"), P("fs", "tp", None), P("fs", "tp"))
    return jax.shard_map(program, mesh=mesh, in_specs=in_specs, out_specs=out_specs, check_vma=False)
```

```python
import functools

import jax
import jax.numpy as jnp
from jax import lax
from jax.experimental import pallas as pl
from jax.experimental.pallas import tpu as pltpu
from jax.sharding import PartitionSpec as P


def normalize(rows):
    values = rows.astype(jnp.float32)
    return (values * lax.rsqrt(jnp.mean(values * values, axis=-1, keepdims=True) + 1e-06)).astype(
        jnp.bfloat16
    )


def local(tokens, routes, route_weight, gain, gate_weight, up_weight, down_weight):
    fs_count = lax.axis_size("fs")
    tp_count = lax.axis_size("tp")
    gain_rows = gain[None, :, None]
    gate_new = (gain_rows * gate_weight).astype(jnp.bfloat16)
    up_new = (gain_rows * up_weight).astype(jnp.bfloat16)
    gate_out, up_out = (
        lax.all_to_all(gate_new, "fs", split_axis=0, concat_axis=1, tiled=True),
        lax.all_to_all(up_new, "fs", split_axis=0, concat_axis=1, tiled=True),
    )
    down_out = lax.all_to_all(
        down_weight.astype(jnp.bfloat16), "fs", split_axis=0, concat_axis=2, tiled=True
    )
    tok_rows, top = routes.shape
    capacity = min(tok_rows, max(2, 3 * tok_rows * top // (2 * fs_count)))
    flat = routes.reshape(-1)
    count = flat.shape[0]
    hits = (flat[:, None] == jnp.arange(fs_count, dtype=jnp.int32)[None, :]).astype(jnp.int32)
    ranks = jnp.sum((jnp.cumsum(hits, axis=0) - 1) * hits, axis=1)
    slots = flat * capacity + ranks
    source = jnp.full((fs_count * capacity,), count, jnp.int32)
    source = source.at[slots].set(jnp.arange(count, dtype=jnp.int32))
    filled = (source < count)[:, None]
    row_of = jnp.minimum(source // top, tok_rows - 1)
    whole = lax.all_gather(tokens, "tp", axis=1, tiled=True)
    normed = normalize(whole)
    packed = jnp.where(filled, normed[row_of], jnp.zeros((), jnp.bfloat16))
    arrived = lax.all_to_all(
        packed.reshape(fs_count, capacity, -1), "fs", split_axis=0, concat_axis=0, tiled=True
    )
    arrived = arrived.reshape(fs_count * capacity, -1)
    gate_act = jnp.dot(arrived, gate_out[0], preferred_element_type=jnp.float32)
    up_act = jnp.dot(arrived, up_out[0], preferred_element_type=jnp.float32)
    hidden = (jax.nn.silu(gate_act) * up_act).astype(jnp.bfloat16)
    slot_rows = hidden.shape[0]
    unit_rows = down_out.shape[1]
    hidden_all = lax.all_gather(hidden, "tp", axis=1, tiled=True)
    column_block = lax.all_to_all(
        down_out[0].reshape(unit_rows, tp_count, -1), "tp", split_axis=1, concat_axis=0, tiled=True
    )
    column_block = column_block.reshape(tp_count, unit_rows, -1)
    hidden_blocks = hidden_all.reshape(slot_rows, tp_count, unit_rows)
    partial_value = jnp.einsum(
        "sju,jud->sjd", hidden_blocks, column_block, preferred_element_type=jnp.float32
    ).astype(jnp.bfloat16)
    expert_out = jnp.sum(partial_value, axis=1, dtype=jnp.float32).astype(jnp.bfloat16)
    returned = lax.all_to_all(
        expert_out.reshape(fs_count, capacity, -1), "fs", split_axis=0, concat_axis=0, tiled=True
    )
    returned = returned.reshape(fs_count * capacity, -1)
    picked = returned[slots].reshape(tok_rows, top, -1)
    share = route_weight / jnp.sum(route_weight, axis=1, keepdims=True)
    mixed = jnp.sum(share[:, :, None] * picked.astype(jnp.float32), axis=1).astype(jnp.bfloat16)
    return (gate_out, up_out, down_out, mixed)


MESH = pl.DeviceIdType.MESH
VMEM_BYTES = 67043328


def flip(index, mask):
    other = index
    bit = 1
    while bit <= mask:
        if mask & bit:
            other = other + (1 - 2 * lax.rem(lax.div(index, bit), 2)) * bit
        bit *= 2
    return other


def serve_kernel(
    fs, tp, cap,
    routes_ref, rw_ref, gain_ref, tokens_hbm, gw_hbm, uw_hbm, dw_hbm,
    gat, upw, dn, r, rc, picks_ref, share_ref,
    tokens_ref, gw, uw, dw, gsend, usend, dsend,
    psend, fsend, ftoks, rsend, froutes, ssend, fshares, x, n, h, wd, y, fpicks, fweights, col, whole,
    load_sem,
    out, w_r, t_r, p_r, xf_r, h_r, wd_r, y_s, y_r, met, c_r, m_r,
):
    me = lax.axis_index("fs")
    mt = lax.axis_index("tp")
    toks, cols = tokens_ref.shape
    rows = gw.shape[1]
    units = gw.shape[2]
    each = cols // rows
    slots = fs * cap
    half = fs // 2
    side = lax.div(me, half)
    bridge = half | half // 2
    across = flip(me, bridge)
    outer = (me < fs // 4) | (me >= fs - fs // 4)
    near = list(range(half - 1, 0, -1))
    far = [flip(me, i) for i in range(fs - 1, half - 1, -1)]
    homeward = [jnp.where(side == 1, q, fs - 1 - q) for q in range(half)]
    links = [(i, 0) for i in [1 << b for b in range(half.bit_length() - 1)] + [bridge]]
    links += [(0, 1 << b) for b in range(tp.bit_length() - 1)]
    direct = [1] + list(range(2, tp, 2))
    relayed = list(range(2, tp, 2))

    loads = [
        pltpu.make_async_copy(src, dst, load_sem.at[k])
        for k, (src, dst) in enumerate(
            ((gw_hbm, gw), (uw_hbm, uw), (dw_hbm, dw), (tokens_hbm, tokens_ref))
        )
    ]
    for load in loads[3:] + loads[:3]:
        load.start()

    barrier = pltpu.get_barrier_semaphore()

    def greet(sem):
        for i, j in links:
            pl.semaphore_signal(
                sem, inc=1, device_id=(flip(me, i), flip(mt, j)), device_id_type=MESH
            )

    r[...] = jnp.zeros(r.shape, r.dtype)
    rc[...] = jnp.zeros(rc.shape, rc.dtype)
    greet(barrier)

    def remote(src, dst, s, d, device):
        return pltpu.make_async_remote_copy(
            src_ref=src, dst_ref=dst, send_sem=s, recv_sem=d, device_id=device, device_id_type=MESH
        )

    def drain(ref, sem):
        pltpu.make_async_copy(ref, ref, sem).wait()

    def send(*args):
        copy = remote(*args)
        copy.start()
        return copy

    earlier = lax.broadcasted_iota(jnp.int32, (toks, toks), 0) < lax.broadcasted_iota(
        jnp.int32, (toks, toks), 1
    )
    earlier = jnp.where(earlier, 1.0, 0.0).astype(jnp.bfloat16)
    place = lax.broadcasted_iota(jnp.int32, (cap, toks), 0).astype(jnp.float32)

    def ranks(one, two, lowest):
        expert = lax.broadcasted_iota(jnp.int32, (fs, toks), 0) + lowest
        member = (expert == one) | (expert == two)
        rank = jnp.dot(
            jnp.where(member, 1.0, 0.0).astype(jnp.bfloat16), earlier,
            preferred_element_type=jnp.float32,
        )
        return jnp.where(member, rank, -1.0)

    def pack(rank, rows_of, into):
        for e in range(half):
            hit = jnp.where(place == rank[e:e + 1, :], 1.0, 0.0).astype(jnp.bfloat16)
            into[e] = jnp.dot(hit, rows_of, preferred_element_type=jnp.float32).astype(jnp.bfloat16)

    first, second = routes_ref[0:1, :], routes_ref[1:2, :]
    rsend[0:2, :] = routes_ref[...]
    ssend[0:2, :] = rw_ref[...] / (rw_ref[0:1, :] + rw_ref[1:2, :])
    rank = ranks(first, second, side * half)
    loads[3].wait()
    pack(rank, tokens_ref[...], psend)
    x[mt, me] = psend[lax.rem(me, half)]

    pl.semaphore_wait(barrier, len(links))
    greet(met.at[0])
    crossing = [
        send(rsend, froutes, out.at[0], t_r.at[0], (across, mt)),
        send(ssend, fshares, out.at[0], t_r.at[2], (across, mt)),
        send(tokens_ref, ftoks, out.at[0], t_r.at[1], (across, mt)),
    ]
    pl.semaphore_wait(met.at[0], len(links))
    greet(met.at[1])
    pl.semaphore_wait(met.at[1], len(links))

    def dispatch(buf, block, base):
        for i in near:
            peer = flip(me, i)
            send(
                buf.at[lax.rem(peer, half)], x.at[mt, block], out.at[0], p_r.at[base],
                (peer, mt),
            )

    def forward(i, apart):
        block = flip(me, i ^ bridge if apart else i)
        for j in direct:
            send(
                x.at[mt, block], x.at[mt, block], out.at[0], xf_r.at[j - 1, apart], (me, flip(mt, j))
            )

    dispatch(psend, me, 0)
    forward(0, 0)

    gain = jnp.broadcast_to(gain_ref[...], (units, rows)).T
    placed = {}
    held = {}
    for k, (raw, buf, dst) in enumerate(((gw, gsend, gat), (uw, usend, upw), (dw, dsend, dn))):
        loads[k].wait()
        for e in range(fs):
            buf[e] = (gain * raw[e] if k < 2 else raw[e]).astype(jnp.bfloat16)
        target = dst.at[me] if k < 2 else dst.at[:, pl.ds(pl.multiple_of(me * rows, rows), rows)]
        held[k] = []
        base = 0 if k == 0 else 2 if k == 1 else 3 + half
        for i in near:
            peer = flip(me, i)
            placed[k, i] = remote(buf.at[peer], target, out.at[0], w_r.at[base], (peer, mt))
            if k == 0:
                placed[k, i].start()
        for v, peer in enumerate(far):
            arrived = base + 1 + (v if k else 0)
            copy = remote(buf.at[peer], target, out.at[0], w_r.at[arrived], (peer, mt))
            pl.when(jnp.logical_not(outer))(copy.start)
            held[k].append((outer, copy))
        if k < 2:
            dst[me] = buf[me]
        else:
            dst[:, pl.ds(pl.multiple_of(me * rows, rows), rows)] = buf[me]

    def release(k):
        for when, copy in held[k]:
            pl.when(when)(copy.start)

    for copy in crossing:
        copy.wait_recv()
    pack(ranks(froutes[0:1, :], froutes[1:2, :], side * half), ftoks[...], fsend)
    x[mt, across] = fsend[lax.rem(me, half)]
    dispatch(fsend, across, 1)
    forward(0, 1)
    for k in (2, 1):
        for i in near:
            placed[k, i].start()
    release(0)
    release(1)
    for apart in range(2):
        drain(psend.at[pl.ds(0, half - 1)], p_r.at[apart])
        for i in near:
            forward(i, apart)

    for v in range(2):
        first_block = pl.multiple_of((1 - side if v else side) * half, half)
        for j in relayed:
            landed = x.at[flip(mt, j), pl.ds(first_block, half)]
            drain(landed, xf_r.at[j - 1, v])
            send(landed, landed, out.at[0], xf_r.at[j, v], (me, flip(mt, 1)))

    def gather(apart, steps):
        for v in steps:
            if apart:
                drain(dsend.at[0], w_r.at[4 + half + v])
            elif v == 0:
                drain(dsend.at[pl.ds(0, half - 1)], w_r.at[3 + half])
            piece = far[v] if apart else flip(me, v)
            owner, part = lax.rem(piece, tp), lax.div(piece, tp)
            block = dn.at[:, pl.ds(pl.multiple_of(piece * rows, rows), rows)]
            landing = wd_r.at[apart]
            stays = pltpu.make_async_copy(block, wd.at[mt, part], landing)
            goes = remote(block, wd.at[mt, part], out.at[0], landing, (me, owner))
            pl.when(owner == mt)(stays.start)
            pl.when(owner != mt)(goes.start)

    def choose(one, two, lowest, experts, shares, picks, weights):
        rank = ranks(one, two, lowest)
        hits = [jnp.where(place == rank[e:e + 1, :], 1.0, 0.0) for e in range(experts)]
        for k, named in enumerate((one, two)):
            picked = jnp.concatenate(
                [jnp.where(named == e + lowest, hits[e], 0.0) for e in range(experts)], axis=0
            )
            picks[k] = picked.T.astype(jnp.bfloat16)
            weights[k] = jnp.broadcast_to(shares[k:k + 1, :], (toks, toks)).T

    choose(first, second, 0, fs, ssend, picks_ref, share_ref)
    choose(
        froutes[0:1, :], froutes[1:2, :], side * half, half, fshares, fpicks, fweights
    )

    for v in range(2):
        for j in range(1, tp, 2):
            drain(x.at[0, pl.ds(0, half)], xf_r.at[j - 1, v])

    for s in range(fs):
        total = jnp.zeros((cap, 1), jnp.float32)
        for j in range(tp):
            value = x[j, s].astype(jnp.float32)
            total = total + jnp.sum(value * value, axis=-1, keepdims=True)
        scale = lax.rsqrt(total / (tp * cols) + 1e-06)
        for j in range(tp):
            normed = (x[j, s].astype(jnp.float32) * scale).astype(jnp.bfloat16)
            for part in range(each):
                n[j * each + part, s * cap:(s + 1) * cap] = normed[:, part * rows:(part + 1) * rows]

    def activate(k, dst):
        base = 0 if k == 0 else 2
        drain(dst.at[pl.ds(0, half - 1)], w_r.at[base])
        pieces = [me] + [flip(me, i) for i in near] + far
        act = jnp.zeros((slots, units), jnp.float32)
        for v, piece in enumerate(pieces):
            if k == 0 and v == half:
                drain(dst.at[pl.ds(0, half)], w_r.at[base + 1])
            if k == 1 and v >= half:
                drain(dst.at[0], w_r.at[base + 1 + v - half])
            act = act + jnp.dot(n[piece], dst[piece], preferred_element_type=jnp.float32)
        return act

    gate_act = activate(0, gat)
    gate_act = gate_act / (1.0 + jnp.exp(-gate_act))
    gather(0, range(half))
    up_act = activate(1, upw)
    h[mt] = (gate_act * up_act).astype(jnp.bfloat16)
    shared = {j: send(h.at[mt], h.at[mt], out.at[0], h_r.at[j - 1], (me, flip(mt, j))) for j in direct}
    release(2)
    for j in relayed:
        shared[j].wait_recv()
        source = flip(mt, j)
        shared[j + 1] = send(
            h.at[source], h.at[source], out.at[0], h_r.at[j], (me, flip(mt, 1))
        )

    moves = []

    def give_back(late):
        first_part = (1 - side if late else side) * (each // 2)
        drain(wd.at[:, pl.ds(0, each // 2)], wd_r.at[late])
        for q in range(each // 2):
            part = first_part + q
            result = jnp.zeros((slots, rows), jnp.float32)
            for j in range(tp):
                term = jnp.dot(h[j], wd[j, part], preferred_element_type=jnp.float32)
                result = result + term.astype(jnp.bfloat16).astype(jnp.float32)
            v = late * (each // 2) + q
            y[v] = result.astype(jnp.bfloat16).reshape(fs, cap, rows)
            piece = part * tp + mt
            home, slot = lax.div(piece, each), lax.rem(piece, each)
            if late:
                for peer in homeward:
                    send(y.at[v, peer], r.at[slot, me], out.at[0], y_r.at[1], (peer, home))
            else:
                mine = lax.rem(me, half)
                for i in near:
                    peer = flip(me, i)
                    send(y.at[v, flip(me, i ^ bridge)], col.at[q, mine], out.at[0], c_r.at[0], (peer, mt))
                col[q, mine] = y[v, across]
            for i in near:
                peer = flip(me, i)
                send(y.at[v, peer], r.at[slot, me], out.at[0], y_r.at[0], (peer, home))
            stays = pltpu.make_async_copy(y.at[v, me], r.at[slot, me], y_r.at[0])
            goes = remote(y.at[v, me], r.at[slot, me], y_s.at[v], y_r.at[0], (me, home))
            pl.when(home == mt)(stays.start)
            pl.when(home != mt)(goes.start)
            moves.append((home != mt, goes))

    def combine():
        waiting = []
        for _ in range(each // 2):
            drain(col.at[0, pl.ds(0, half - 1)], c_r.at[0])
        for q in range(each // 2):
            back = col[q].reshape(half * cap, rows)
            total = jnp.zeros((toks, rows), jnp.float32)
            for k in range(2):
                term = jnp.dot(fpicks[k], back, preferred_element_type=jnp.float32)
                total = total + fweights[k][:, 0:1] * term
            whole[q] = total.astype(jnp.bfloat16)
            piece = (side * (each // 2) + q) * tp + mt
            home, slot = lax.div(piece, each), lax.rem(piece, each)
            copy = remote(whole.at[q], rc.at[slot], out.at[0], m_r.at[0], (across, home))
            copy.start()
        return waiting

    for j, copy in shared.items():
        if j % 2:
            copy.wait_recv()
    give_back(0)
    gather(1, range(half))
    held[3] = combine()
    release(3)
    give_back(1)

    drain(r.at[:, pl.ds(0, half)], y_r.at[0])
    alike = lax.div(mt, tp // 2) == side

    @pl.when(alike)
    def _():
        drain(r.at[:, pl.ds(0, half)], y_r.at[1])

    @pl.when(jnp.logical_not(alike))
    def _():
        drain(rc, m_r.at[0])

    for copy in crossing:
        copy.wait_send()
    for k, buf in enumerate((gsend, usend, dsend)):
        drain(buf.at[pl.ds(0, fs - 1)], out.at[0])
    for _ in range(2):
        drain(psend.at[pl.ds(0, half - 1)], out.at[0])
    for _ in range(tp - 1):
        drain(x.at[0], out.at[0])
    drain(h.at[pl.ds(0, tp - 1)], out.at[0])
    for _ in range(tp - 1):
        drain(wd.at[0], out.at[0])
    drain(y.at[pl.ds(0, each // 2), pl.ds(0, half - 1)], out.at[0])
    drain(y.at[pl.ds(0, each // 2), pl.ds(0, fs - 1)], out.at[0])
    drain(y.at[pl.ds(0, each // 2), pl.ds(0, half - 1)], out.at[0])
    drain(whole, out.at[0])
    for away, goes in moves:
        pl.when(away)(goes.wait_send)


def mix_kernel(gat, upw, dn, r, rc, picks_ref, share_ref, gate_hbm, up_hbm, down_hbm, mixed_hbm, mixed, sem):
    outs = [
        pltpu.make_async_copy(src, dst, sem.at[k])
        for k, (src, dst) in enumerate(
            ((gat, gate_hbm), (upw, up_hbm), (dn, down_hbm), (mixed, mixed_hbm))
        )
    ]
    for copy in outs[:3]:
        copy.start()
    each, fs, cap, rows = r.shape
    for slot in range(each):
        back = r[slot].reshape(fs * cap, rows)
        total = rc[slot].astype(jnp.float32)
        for k in range(2):
            term = jnp.dot(picks_ref[k], back, preferred_element_type=jnp.float32)
            total = total + share_ref[k][:, 0:1] * term
        mixed[:, slot * rows:(slot + 1) * rows] = total.astype(jnp.bfloat16)
    outs[3].start()
    for copy in outs:
        copy.wait()


def fused(tokens, routes, route_weight, gain, gate_weight, up_weight, down_weight):
    fs = lax.axis_size("fs")
    tp = lax.axis_size("tp")
    toks, cols = tokens.shape
    top = routes.shape[1]
    cap = capacity_of(toks, top, fs)
    rows, units = gate_weight.shape[1:]
    each = cols // rows
    slots = fs * cap
    bf, f32 = jnp.bfloat16, jnp.float32
    hbm, vmem = pl.BlockSpec(memory_space=pltpu.HBM), pl.BlockSpec(memory_space=pltpu.VMEM)
    dma = pltpu.SemaphoreType.DMA
    kept = 2 * (3 * fs * rows * units + slots * cols + toks * cols + top * toks * slots) + 4 * top * toks * toks
    landed = pl.pallas_call(
        functools.partial(serve_kernel, fs, tp, cap),
        out_shape=(
            pltpu.VMEM((fs, rows, units), bf),
            pltpu.VMEM((fs, rows, units), bf),
            pltpu.VMEM((units, fs * rows), bf),
            pltpu.VMEM((each, fs, cap, rows), bf),
            pltpu.VMEM((each, toks, rows), bf),
            pltpu.VMEM((top, toks, slots), bf),
            pltpu.VMEM((top, toks, toks), f32),
        ),
        in_specs=[vmem] * 3 + [hbm] * 4,
        out_specs=(vmem,) * 7,
        scratch_shapes=[
            pltpu.VMEM((toks, cols), bf),
            pltpu.VMEM((fs, rows, units), f32),
            pltpu.VMEM((fs, rows, units), f32),
            pltpu.VMEM((fs, units, rows), f32),
            pltpu.VMEM((fs, rows, units), bf),
            pltpu.VMEM((fs, rows, units), bf),
            pltpu.VMEM((fs, units, rows), bf),
            pltpu.VMEM((fs // 2, cap, cols), bf),
            pltpu.VMEM((fs // 2, cap, cols), bf),
            pltpu.VMEM((toks, cols), bf),
            pltpu.VMEM((8, toks), jnp.int32),
            pltpu.VMEM((8, toks), jnp.int32),
            pltpu.VMEM((8, toks), f32),
            pltpu.VMEM((8, toks), f32),
            pltpu.VMEM((tp, fs, cap, cols), bf),
            pltpu.VMEM((fs, slots, rows), bf),
            pltpu.VMEM((tp, slots, units), bf),
            pltpu.VMEM((tp, each, units, rows), bf),
            pltpu.VMEM((each, fs, cap, rows), bf),
            pltpu.VMEM((top, toks, slots // 2), bf),
            pltpu.VMEM((top, toks, toks), f32),
            pltpu.VMEM((each // 2, fs // 2, cap, rows), bf),
            pltpu.VMEM((each // 2, toks, rows), bf),
            dma((4,)),
            dma((1,)), dma((fs + 4,)), dma((3,)), dma((2,)), dma((tp - 1, 2)), dma((tp - 1,)),
            dma((2,)), dma((each,)), dma((2,)),
            pltpu.SemaphoreType.REGULAR((2,)),
            dma((1,)), dma((1,)),
        ],
        compiler_params=pltpu.CompilerParams(
            collective_id=0, has_side_effects=True, vmem_limit_bytes=VMEM_BYTES - kept - 2**16
        ),
        name="serve",
    )(routes.T, route_weight.T, gain.reshape(1, -1), tokens, gate_weight, up_weight, down_weight)
    gate, up, down, mixed = pl.pallas_call(
        mix_kernel,
        out_shape=(
            jax.ShapeDtypeStruct((fs, rows, units), bf),
            jax.ShapeDtypeStruct((fs, rows, units), bf),
            jax.ShapeDtypeStruct((units, fs * rows), bf),
            jax.ShapeDtypeStruct((toks, cols), bf),
        ),
        in_specs=[vmem] * 7,
        out_specs=(hbm,) * 4,
        scratch_shapes=[pltpu.VMEM((toks, cols), bf), dma((4,))],
        compiler_params=pltpu.CompilerParams(vmem_limit_bytes=16 * 2**20),
        name="mix",
    )(*landed)
    return (
        gate.reshape(1, fs * rows, units),
        up.reshape(1, fs * rows, units),
        down[None],
        mixed,
    )


def capacity_of(tok_rows, top, fs_count):
    return min(tok_rows, max(2, 3 * tok_rows * top // (2 * fs_count)))


def one_kernel(fs, tp, toks, top, experts, rows, units, cols):
    cap = capacity_of(toks, top, fs)
    powers = fs & (fs - 1) == 0 and tp & (tp - 1) == 0 and fs >= 4 and tp >= 2
    small = fs <= 16 and tp <= 8 and top == 2 and experts == fs
    tiled = cap % 16 == 0 and rows % 128 == 0 and units % 128 == 0 and toks % 128 == 0
    return powers and small and tiled and cols % (2 * rows) == 0 and fs * rows == tp * cols


def program(*args):
    tokens, routes, gate_weight = args[0], args[1], args[4]
    experts, rows, units = gate_weight.shape
    if one_kernel(
        lax.axis_size("fs"), lax.axis_size("tp"), tokens.shape[0], routes.shape[1],
        experts, rows, units, tokens.shape[1],
    ):
        return fused(*args)
    return local(*args)


def solution(mesh):
    in_specs = (
        P("fs", "tp"),
        P("fs", None),
        P("fs", None),
        P("fs"),
        P(None, "fs", "tp"),
        P(None, "fs", "tp"),
        P(None, "tp", "fs"),
    )
    out_specs = (P("fs", None, "tp"), P("fs", None, "tp"), P("fs", "tp", None), P("fs", "tp"))
    return jax.shard_map(program, mesh=mesh, in_specs=in_specs, out_specs=out_specs, check_vma=False)
```

```python
import functools

import jax
import jax.numpy as jnp
from jax import lax
from jax.experimental import pallas as pl
from jax.experimental.pallas import tpu as pltpu
from jax.sharding import PartitionSpec as P


def normalize(rows):
    values = rows.astype(jnp.float32)
    return (values * lax.rsqrt(jnp.mean(values * values, axis=-1, keepdims=True) + 1e-06)).astype(
        jnp.bfloat16
    )


def local(tokens, routes, route_weight, gain, gate_weight, up_weight, down_weight):
    fs_count = lax.axis_size("fs")
    tp_count = lax.axis_size("tp")
    gain_rows = gain[None, :, None]
    gate_new = (gain_rows * gate_weight).astype(jnp.bfloat16)
    up_new = (gain_rows * up_weight).astype(jnp.bfloat16)
    gate_out, up_out = (
        lax.all_to_all(gate_new, "fs", split_axis=0, concat_axis=1, tiled=True),
        lax.all_to_all(up_new, "fs", split_axis=0, concat_axis=1, tiled=True),
    )
    down_out = lax.all_to_all(
        down_weight.astype(jnp.bfloat16), "fs", split_axis=0, concat_axis=2, tiled=True
    )
    tok_rows, top = routes.shape
    capacity = min(tok_rows, max(2, 3 * tok_rows * top // (2 * fs_count)))
    flat = routes.reshape(-1)
    count = flat.shape[0]
    hits = (flat[:, None] == jnp.arange(fs_count, dtype=jnp.int32)[None, :]).astype(jnp.int32)
    ranks = jnp.sum((jnp.cumsum(hits, axis=0) - 1) * hits, axis=1)
    slots = flat * capacity + ranks
    source = jnp.full((fs_count * capacity,), count, jnp.int32)
    source = source.at[slots].set(jnp.arange(count, dtype=jnp.int32))
    filled = (source < count)[:, None]
    row_of = jnp.minimum(source // top, tok_rows - 1)
    whole = lax.all_gather(tokens, "tp", axis=1, tiled=True)
    normed = normalize(whole)
    packed = jnp.where(filled, normed[row_of], jnp.zeros((), jnp.bfloat16))
    arrived = lax.all_to_all(
        packed.reshape(fs_count, capacity, -1), "fs", split_axis=0, concat_axis=0, tiled=True
    )
    arrived = arrived.reshape(fs_count * capacity, -1)
    gate_act = jnp.dot(arrived, gate_out[0], preferred_element_type=jnp.float32)
    up_act = jnp.dot(arrived, up_out[0], preferred_element_type=jnp.float32)
    hidden = (jax.nn.silu(gate_act) * up_act).astype(jnp.bfloat16)
    slot_rows = hidden.shape[0]
    unit_rows = down_out.shape[1]
    hidden_all = lax.all_gather(hidden, "tp", axis=1, tiled=True)
    column_block = lax.all_to_all(
        down_out[0].reshape(unit_rows, tp_count, -1), "tp", split_axis=1, concat_axis=0, tiled=True
    )
    column_block = column_block.reshape(tp_count, unit_rows, -1)
    hidden_blocks = hidden_all.reshape(slot_rows, tp_count, unit_rows)
    partial_value = jnp.einsum(
        "sju,jud->sjd", hidden_blocks, column_block, preferred_element_type=jnp.float32
    ).astype(jnp.bfloat16)
    expert_out = jnp.sum(partial_value, axis=1, dtype=jnp.float32).astype(jnp.bfloat16)
    returned = lax.all_to_all(
        expert_out.reshape(fs_count, capacity, -1), "fs", split_axis=0, concat_axis=0, tiled=True
    )
    returned = returned.reshape(fs_count * capacity, -1)
    picked = returned[slots].reshape(tok_rows, top, -1)
    share = route_weight / jnp.sum(route_weight, axis=1, keepdims=True)
    mixed = jnp.sum(share[:, :, None] * picked.astype(jnp.float32), axis=1).astype(jnp.bfloat16)
    return (gate_out, up_out, down_out, mixed)


MESH = pl.DeviceIdType.MESH
VMEM_BYTES = 67043328


def flip(index, mask):
    other = index
    bit = 1
    while bit <= mask:
        if mask & bit:
            other = other + (1 - 2 * lax.rem(lax.div(index, bit), 2)) * bit
        bit *= 2
    return other


def serve_kernel(
    fs, tp, cap,
    routes_ref, rw_ref, gain_ref, tokens_hbm, gw_hbm, uw_hbm, dw_hbm,
    gat, upw, dn, r, rc, picks_ref, share_ref,
    tokens_ref, gw, uw, dw, gsend, usend, dsend,
    psend, fsend, ftoks, rsend, froutes, ssend, fshares, x, n, h, wd, y, fpicks, fweights, col, whole,
    load_sem,
    out, w_r, t_r, p_r, xf_r, h_r, wd_r, y_s, y_r, met, c_r, m_r,
):
    me = lax.axis_index("fs")
    mt = lax.axis_index("tp")
    toks, cols = tokens_ref.shape
    rows = gw.shape[1]
    units = gw.shape[2]
    each = cols // rows
    slots = fs * cap
    half = fs // 2
    side = lax.div(me, half)
    bridge = half | half // 2
    across = flip(me, bridge)
    outer = (me < fs // 4) | (me >= fs - fs // 4)
    near = list(range(half - 1, 0, -1))
    far = [flip(me, i) for i in range(fs - 1, half - 1, -1)]
    homeward = [jnp.where(side == 1, q, fs - 1 - q) for q in range(half)]
    links = [(i, 0) for i in [1 << b for b in range(half.bit_length() - 1)] + [bridge]]
    links += [(0, 1 << b) for b in range(tp.bit_length() - 1)]
    direct = [1] + list(range(2, tp, 2))
    relayed = list(range(2, tp, 2))

    loads = [
        pltpu.make_async_copy(src, dst, load_sem.at[k])
        for k, (src, dst) in enumerate(
            ((gw_hbm, gw), (uw_hbm, uw), (dw_hbm, dw), (tokens_hbm, tokens_ref))
        )
    ]
    for load in loads[3:] + loads[:3]:
        load.start()

    barrier = pltpu.get_barrier_semaphore()

    def greet(sem):
        for i, j in links:
            pl.semaphore_signal(
                sem, inc=1, device_id=(flip(me, i), flip(mt, j)), device_id_type=MESH
            )

    r[...] = jnp.zeros(r.shape, r.dtype)
    rc[...] = jnp.zeros(rc.shape, rc.dtype)
    greet(barrier)

    def remote(src, dst, s, d, device):
        return pltpu.make_async_remote_copy(
            src_ref=src, dst_ref=dst, send_sem=s, recv_sem=d, device_id=device, device_id_type=MESH
        )

    def drain(ref, sem):
        pltpu.make_async_copy(ref, ref, sem).wait()

    def send(*args):
        copy = remote(*args)
        copy.start()
        return copy

    earlier = lax.broadcasted_iota(jnp.int32, (toks, toks), 0) < lax.broadcasted_iota(
        jnp.int32, (toks, toks), 1
    )
    earlier = jnp.where(earlier, 1.0, 0.0).astype(jnp.bfloat16)
    place = lax.broadcasted_iota(jnp.int32, (cap, toks), 0).astype(jnp.float32)

    def ranks(one, two, lowest):
        expert = lax.broadcasted_iota(jnp.int32, (fs, toks), 0) + lowest
        member = (expert == one) | (expert == two)
        rank = jnp.dot(
            jnp.where(member, 1.0, 0.0).astype(jnp.bfloat16), earlier,
            preferred_element_type=jnp.float32,
        )
        return jnp.where(member, rank, -1.0)

    def pack(rank, rows_of, into):
        for e in range(half):
            hit = jnp.where(place == rank[e:e + 1, :], 1.0, 0.0).astype(jnp.bfloat16)
            into[e] = jnp.dot(hit, rows_of, preferred_element_type=jnp.float32).astype(jnp.bfloat16)

    first, second = routes_ref[0:1, :], routes_ref[1:2, :]
    rsend[0:2, :] = routes_ref[...]
    ssend[0:2, :] = rw_ref[...] / (rw_ref[0:1, :] + rw_ref[1:2, :])
    rank = ranks(first, second, side * half)
    loads[3].wait()
    pack(rank, tokens_ref[...], psend)
    x[mt, me] = psend[lax.rem(me, half)]

    pl.semaphore_wait(barrier, len(links))
    greet(met.at[0])
    crossing = [
        send(rsend, froutes, out.at[0], t_r.at[0], (across, mt)),
        send(ssend, fshares, out.at[0], t_r.at[2], (across, mt)),
        send(tokens_ref, ftoks, out.at[0], t_r.at[1], (across, mt)),
    ]
    pl.semaphore_wait(met.at[0], len(links))
    greet(met.at[1])
    pl.semaphore_wait(met.at[1], len(links))

    def dispatch(buf, block, base):
        for i in near:
            peer = flip(me, i)
            send(
                buf.at[lax.rem(peer, half)], x.at[mt, block], out.at[0], p_r.at[base],
                (peer, mt),
            )

    def forward(i, apart):
        block = flip(me, i ^ bridge if apart else i)
        for j in direct:
            send(
                x.at[mt, block], x.at[mt, block], out.at[0], xf_r.at[j - 1, apart], (me, flip(mt, j))
            )

    dispatch(psend, me, 0)
    forward(0, 0)

    gain = jnp.broadcast_to(gain_ref[...], (units, rows)).T
    placed = {}
    held = {4: []}
    for k, (raw, buf, dst) in enumerate(((gw, gsend, gat), (uw, usend, upw), (dw, dsend, dn))):
        loads[k].wait()
        for e in range(fs):
            buf[e] = (gain * raw[e] if k < 2 else raw[e]).astype(jnp.bfloat16)
        target = dst.at[me] if k < 2 else dst.at[:, pl.ds(pl.multiple_of(me * rows, rows), rows)]
        held[k] = []
        base = 0 if k == 0 else 2 if k == 1 else 3 + half
        for i in near:
            peer = flip(me, i)
            placed[k, i] = remote(buf.at[peer], target, out.at[0], w_r.at[base], (peer, mt))
            if k == 0:
                placed[k, i].start()
        for v, peer in enumerate(far):
            arrived = base + 1 + (v if k else 0)
            copy = remote(buf.at[peer], target, out.at[0], w_r.at[arrived], (peer, mt))
            if k < 2:
                pl.when(jnp.logical_not(outer))(copy.start)
            else:
                pl.when(jnp.logical_not(outer) & (lax.rem(mt, 2) == 0))(copy.start)
                held[4].append((jnp.logical_not(outer) & (lax.rem(mt, 2) == 1), copy))
            held[k].append((outer, copy))
        if k < 2:
            dst[me] = buf[me]
        else:
            dst[:, pl.ds(pl.multiple_of(me * rows, rows), rows)] = buf[me]

    def release(k):
        for when, copy in held[k]:
            pl.when(when)(copy.start)

    for copy in crossing:
        copy.wait_recv()
    pack(ranks(froutes[0:1, :], froutes[1:2, :], side * half), ftoks[...], fsend)
    x[mt, across] = fsend[lax.rem(me, half)]
    dispatch(fsend, across, 1)
    forward(0, 1)
    for k in (2, 1):
        for i in near:
            placed[k, i].start()
    release(0)
    release(1)
    for apart in range(2):
        drain(psend.at[pl.ds(0, half - 1)], p_r.at[apart])
        for i in near:
            forward(i, apart)

    for v in range(2):
        first_block = pl.multiple_of((1 - side if v else side) * half, half)
        for j in relayed:
            landed = x.at[flip(mt, j), pl.ds(first_block, half)]
            drain(landed, xf_r.at[j - 1, v])
            send(landed, landed, out.at[0], xf_r.at[j, v], (me, flip(mt, 1)))

    def gather(apart, steps):
        for v in steps:
            if apart:
                drain(dsend.at[0], w_r.at[4 + half + v])
            elif v == 0:
                drain(dsend.at[pl.ds(0, half - 1)], w_r.at[3 + half])
            piece = far[v] if apart else flip(me, v)
            owner, part = lax.rem(piece, tp), lax.div(piece, tp)
            block = dn.at[:, pl.ds(pl.multiple_of(piece * rows, rows), rows)]
            landing = wd_r.at[apart]
            stays = pltpu.make_async_copy(block, wd.at[mt, part], landing)
            goes = remote(block, wd.at[mt, part], out.at[0], landing, (me, owner))
            pl.when(owner == mt)(stays.start)
            pl.when(owner != mt)(goes.start)

    def choose(one, two, lowest, experts, shares, picks, weights):
        rank = ranks(one, two, lowest)
        hits = [jnp.where(place == rank[e:e + 1, :], 1.0, 0.0) for e in range(experts)]
        for k, named in enumerate((one, two)):
            picked = jnp.concatenate(
                [jnp.where(named == e + lowest, hits[e], 0.0) for e in range(experts)], axis=0
            )
            picks[k] = picked.T.astype(jnp.bfloat16)
            weights[k] = jnp.broadcast_to(shares[k:k + 1, :], (toks, toks)).T

    choose(first, second, 0, fs, ssend, picks_ref, share_ref)
    choose(
        froutes[0:1, :], froutes[1:2, :], side * half, half, fshares, fpicks, fweights
    )

    for v in range(2):
        for j in range(1, tp, 2):
            drain(x.at[0, pl.ds(0, half)], xf_r.at[j - 1, v])

    for s in range(fs):
        total = jnp.zeros((cap, 1), jnp.float32)
        for j in range(tp):
            value = x[j, s].astype(jnp.float32)
            total = total + jnp.sum(value * value, axis=-1, keepdims=True)
        scale = lax.rsqrt(total / (tp * cols) + 1e-06)
        for j in range(tp):
            normed = (x[j, s].astype(jnp.float32) * scale).astype(jnp.bfloat16)
            for part in range(each):
                n[j * each + part, s * cap:(s + 1) * cap] = normed[:, part * rows:(part + 1) * rows]

    def activate(k, dst):
        base = 0 if k == 0 else 2
        drain(dst.at[pl.ds(0, half - 1)], w_r.at[base])
        pieces = [me] + [flip(me, i) for i in near] + far
        act = jnp.zeros((slots, units), jnp.float32)
        for v, piece in enumerate(pieces):
            if k == 0 and v == half:
                drain(dst.at[pl.ds(0, half)], w_r.at[base + 1])
            if k == 1 and v >= half:
                drain(dst.at[0], w_r.at[base + 1 + v - half])
            act = act + jnp.dot(n[piece], dst[piece], preferred_element_type=jnp.float32)
        return act

    release(4)
    gate_act = activate(0, gat)
    gate_act = gate_act / (1.0 + jnp.exp(-gate_act))
    gather(0, range(half))
    up_act = activate(1, upw)
    h[mt] = (gate_act * up_act).astype(jnp.bfloat16)
    shared = {j: send(h.at[mt], h.at[mt], out.at[0], h_r.at[j - 1], (me, flip(mt, j))) for j in direct}
    release(2)
    for j in relayed:
        shared[j].wait_recv()
        source = flip(mt, j)
        shared[j + 1] = send(
            h.at[source], h.at[source], out.at[0], h_r.at[j], (me, flip(mt, 1))
        )

    moves = []

    def give_back(late):
        first_part = (1 - side if late else side) * (each // 2)
        drain(wd.at[:, pl.ds(0, each // 2)], wd_r.at[late])
        for q in range(each // 2):
            part = first_part + q
            result = jnp.zeros((slots, rows), jnp.float32)
            for j in range(tp):
                term = jnp.dot(h[j], wd[j, part], preferred_element_type=jnp.float32)
                result = result + term.astype(jnp.bfloat16).astype(jnp.float32)
            v = late * (each // 2) + q
            y[v] = result.astype(jnp.bfloat16).reshape(fs, cap, rows)
            piece = part * tp + mt
            home, slot = lax.div(piece, each), lax.rem(piece, each)
            if late:
                for peer in homeward:
                    send(y.at[v, peer], r.at[slot, me], out.at[0], y_r.at[1], (peer, home))
            else:
                mine = lax.rem(me, half)
                for i in near:
                    peer = flip(me, i)
                    send(y.at[v, flip(me, i ^ bridge)], col.at[q, mine], out.at[0], c_r.at[0], (peer, mt))
                col[q, mine] = y[v, across]
            for i in near:
                peer = flip(me, i)
                send(y.at[v, peer], r.at[slot, me], out.at[0], y_r.at[0], (peer, home))
            stays = pltpu.make_async_copy(y.at[v, me], r.at[slot, me], y_r.at[0])
            goes = remote(y.at[v, me], r.at[slot, me], y_s.at[v], y_r.at[0], (me, home))
            pl.when(home == mt)(stays.start)
            pl.when(home != mt)(goes.start)
            moves.append((home != mt, goes))

    def combine():
        waiting = []
        for _ in range(each // 2):
            drain(col.at[0, pl.ds(0, half - 1)], c_r.at[0])
        for q in range(each // 2):
            back = col[q].reshape(half * cap, rows)
            total = jnp.zeros((toks, rows), jnp.float32)
            for k in range(2):
                term = jnp.dot(fpicks[k], back, preferred_element_type=jnp.float32)
                total = total + fweights[k][:, 0:1] * term
            whole[q] = total.astype(jnp.bfloat16)
            piece = (side * (each // 2) + q) * tp + mt
            home, slot = lax.div(piece, each), lax.rem(piece, each)
            copy = remote(whole.at[q], rc.at[slot], out.at[0], m_r.at[0], (across, home))
            copy.start()
        return waiting

    for j, copy in shared.items():
        if j % 2:
            copy.wait_recv()
    give_back(0)
    gather(1, range(half))
    held[3] = combine()
    release(3)
    give_back(1)

    drain(r.at[:, pl.ds(0, half)], y_r.at[0])
    alike = lax.div(mt, tp // 2) == side

    @pl.when(alike)
    def _():
        drain(r.at[:, pl.ds(0, half)], y_r.at[1])

    @pl.when(jnp.logical_not(alike))
    def _():
        drain(rc, m_r.at[0])

    for copy in crossing:
        copy.wait_send()
    for k, buf in enumerate((gsend, usend, dsend)):
        drain(buf.at[pl.ds(0, fs - 1)], out.at[0])
    for _ in range(2):
        drain(psend.at[pl.ds(0, half - 1)], out.at[0])
    for _ in range(tp - 1):
        drain(x.at[0], out.at[0])
    drain(h.at[pl.ds(0, tp - 1)], out.at[0])
    for _ in range(tp - 1):
        drain(wd.at[0], out.at[0])
    drain(y.at[pl.ds(0, each // 2), pl.ds(0, half - 1)], out.at[0])
    drain(y.at[pl.ds(0, each // 2), pl.ds(0, fs - 1)], out.at[0])
    drain(y.at[pl.ds(0, each // 2), pl.ds(0, half - 1)], out.at[0])
    drain(whole, out.at[0])
    for away, goes in moves:
        pl.when(away)(goes.wait_send)


def mix_kernel(gat, upw, dn, r, rc, picks_ref, share_ref, gate_hbm, up_hbm, down_hbm, mixed_hbm, mixed, sem):
    outs = [
        pltpu.make_async_copy(src, dst, sem.at[k])
        for k, (src, dst) in enumerate(
            ((gat, gate_hbm), (upw, up_hbm), (dn, down_hbm), (mixed, mixed_hbm))
        )
    ]
    for copy in outs[:3]:
        copy.start()
    each, fs, cap, rows = r.shape
    for slot in range(each):
        back = r[slot].reshape(fs * cap, rows)
        total = rc[slot].astype(jnp.float32)
        for k in range(2):
            term = jnp.dot(picks_ref[k], back, preferred_element_type=jnp.float32)
            total = total + share_ref[k][:, 0:1] * term
        mixed[:, slot * rows:(slot + 1) * rows] = total.astype(jnp.bfloat16)
    outs[3].start()
    for copy in outs:
        copy.wait()


def fused(tokens, routes, route_weight, gain, gate_weight, up_weight, down_weight):
    fs = lax.axis_size("fs")
    tp = lax.axis_size("tp")
    toks, cols = tokens.shape
    top = routes.shape[1]
    cap = capacity_of(toks, top, fs)
    rows, units = gate_weight.shape[1:]
    each = cols // rows
    slots = fs * cap
    bf, f32 = jnp.bfloat16, jnp.float32
    hbm, vmem = pl.BlockSpec(memory_space=pltpu.HBM), pl.BlockSpec(memory_space=pltpu.VMEM)
    dma = pltpu.SemaphoreType.DMA
    kept = 2 * (3 * fs * rows * units + slots * cols + toks * cols + top * toks * slots) + 4 * top * toks * toks
    landed = pl.pallas_call(
        functools.partial(serve_kernel, fs, tp, cap),
        out_shape=(
            pltpu.VMEM((fs, rows, units), bf),
            pltpu.VMEM((fs, rows, units), bf),
            pltpu.VMEM((units, fs * rows), bf),
            pltpu.VMEM((each, fs, cap, rows), bf),
            pltpu.VMEM((each, toks, rows), bf),
            pltpu.VMEM((top, toks, slots), bf),
            pltpu.VMEM((top, toks, toks), f32),
        ),
        in_specs=[vmem] * 3 + [hbm] * 4,
        out_specs=(vmem,) * 7,
        scratch_shapes=[
            pltpu.VMEM((toks, cols), bf),
            pltpu.VMEM((fs, rows, units), f32),
            pltpu.VMEM((fs, rows, units), f32),
            pltpu.VMEM((fs, units, rows), f32),
            pltpu.VMEM((fs, rows, units), bf),
            pltpu.VMEM((fs, rows, units), bf),
            pltpu.VMEM((fs, units, rows), bf),
            pltpu.VMEM((fs // 2, cap, cols), bf),
            pltpu.VMEM((fs // 2, cap, cols), bf),
            pltpu.VMEM((toks, cols), bf),
            pltpu.VMEM((8, toks), jnp.int32),
            pltpu.VMEM((8, toks), jnp.int32),
            pltpu.VMEM((8, toks), f32),
            pltpu.VMEM((8, toks), f32),
            pltpu.VMEM((tp, fs, cap, cols), bf),
            pltpu.VMEM((fs, slots, rows), bf),
            pltpu.VMEM((tp, slots, units), bf),
            pltpu.VMEM((tp, each, units, rows), bf),
            pltpu.VMEM((each, fs, cap, rows), bf),
            pltpu.VMEM((top, toks, slots // 2), bf),
            pltpu.VMEM((top, toks, toks), f32),
            pltpu.VMEM((each // 2, fs // 2, cap, rows), bf),
            pltpu.VMEM((each // 2, toks, rows), bf),
            dma((4,)),
            dma((1,)), dma((fs + 4,)), dma((3,)), dma((2,)), dma((tp - 1, 2)), dma((tp - 1,)),
            dma((2,)), dma((each,)), dma((2,)),
            pltpu.SemaphoreType.REGULAR((2,)),
            dma((1,)), dma((1,)),
        ],
        compiler_params=pltpu.CompilerParams(
            collective_id=0, has_side_effects=True, vmem_limit_bytes=VMEM_BYTES - kept - 2**16
        ),
        name="serve",
    )(routes.T, route_weight.T, gain.reshape(1, -1), tokens, gate_weight, up_weight, down_weight)
    gate, up, down, mixed = pl.pallas_call(
        mix_kernel,
        out_shape=(
            jax.ShapeDtypeStruct((fs, rows, units), bf),
            jax.ShapeDtypeStruct((fs, rows, units), bf),
            jax.ShapeDtypeStruct((units, fs * rows), bf),
            jax.ShapeDtypeStruct((toks, cols), bf),
        ),
        in_specs=[vmem] * 7,
        out_specs=(hbm,) * 4,
        scratch_shapes=[pltpu.VMEM((toks, cols), bf), dma((4,))],
        compiler_params=pltpu.CompilerParams(vmem_limit_bytes=16 * 2**20),
        name="mix",
    )(*landed)
    return (
        gate.reshape(1, fs * rows, units),
        up.reshape(1, fs * rows, units),
        down[None],
        mixed,
    )


def capacity_of(tok_rows, top, fs_count):
    return min(tok_rows, max(2, 3 * tok_rows * top // (2 * fs_count)))


def one_kernel(fs, tp, toks, top, experts, rows, units, cols):
    cap = capacity_of(toks, top, fs)
    powers = fs & (fs - 1) == 0 and tp & (tp - 1) == 0 and fs >= 4 and tp >= 2
    small = fs <= 16 and tp <= 8 and top == 2 and experts == fs
    tiled = cap % 16 == 0 and rows % 128 == 0 and units % 128 == 0 and toks % 128 == 0
    return powers and small and tiled and cols % (2 * rows) == 0 and fs * rows == tp * cols


def program(*args):
    tokens, routes, gate_weight = args[0], args[1], args[4]
    experts, rows, units = gate_weight.shape
    if one_kernel(
        lax.axis_size("fs"), lax.axis_size("tp"), tokens.shape[0], routes.shape[1],
        experts, rows, units, tokens.shape[1],
    ):
        return fused(*args)
    return local(*args)


def solution(mesh):
    in_specs = (
        P("fs", "tp"),
        P("fs", None),
        P("fs", None),
        P("fs"),
        P(None, "fs", "tp"),
        P(None, "fs", "tp"),
        P(None, "tp", "fs"),
    )
    out_specs = (P("fs", None, "tp"), P("fs", None, "tp"), P("fs", "tp", None), P("fs", "tp"))
    return jax.shard_map(program, mesh=mesh, in_specs=in_specs, out_specs=out_specs, check_vma=False)
```

```python
import functools

import jax
import jax.numpy as jnp
from jax import lax
from jax.experimental import pallas as pl
from jax.experimental.pallas import tpu as pltpu
from jax.sharding import PartitionSpec as P


def normalize(rows):
    values = rows.astype(jnp.float32)
    return (values * lax.rsqrt(jnp.mean(values * values, axis=-1, keepdims=True) + 1e-06)).astype(
        jnp.bfloat16
    )


def local(tokens, routes, route_weight, gain, gate_weight, up_weight, down_weight):
    fs_count = lax.axis_size("fs")
    tp_count = lax.axis_size("tp")
    gain_rows = gain[None, :, None]
    gate_new = (gain_rows * gate_weight).astype(jnp.bfloat16)
    up_new = (gain_rows * up_weight).astype(jnp.bfloat16)
    gate_out, up_out = (
        lax.all_to_all(gate_new, "fs", split_axis=0, concat_axis=1, tiled=True),
        lax.all_to_all(up_new, "fs", split_axis=0, concat_axis=1, tiled=True),
    )
    down_out = lax.all_to_all(
        down_weight.astype(jnp.bfloat16), "fs", split_axis=0, concat_axis=2, tiled=True
    )
    tok_rows, top = routes.shape
    capacity = min(tok_rows, max(2, 3 * tok_rows * top // (2 * fs_count)))
    flat = routes.reshape(-1)
    count = flat.shape[0]
    hits = (flat[:, None] == jnp.arange(fs_count, dtype=jnp.int32)[None, :]).astype(jnp.int32)
    ranks = jnp.sum((jnp.cumsum(hits, axis=0) - 1) * hits, axis=1)
    slots = flat * capacity + ranks
    source = jnp.full((fs_count * capacity,), count, jnp.int32)
    source = source.at[slots].set(jnp.arange(count, dtype=jnp.int32))
    filled = (source < count)[:, None]
    row_of = jnp.minimum(source // top, tok_rows - 1)
    whole = lax.all_gather(tokens, "tp", axis=1, tiled=True)
    normed = normalize(whole)
    packed = jnp.where(filled, normed[row_of], jnp.zeros((), jnp.bfloat16))
    arrived = lax.all_to_all(
        packed.reshape(fs_count, capacity, -1), "fs", split_axis=0, concat_axis=0, tiled=True
    )
    arrived = arrived.reshape(fs_count * capacity, -1)
    gate_act = jnp.dot(arrived, gate_out[0], preferred_element_type=jnp.float32)
    up_act = jnp.dot(arrived, up_out[0], preferred_element_type=jnp.float32)
    hidden = (jax.nn.silu(gate_act) * up_act).astype(jnp.bfloat16)
    slot_rows = hidden.shape[0]
    unit_rows = down_out.shape[1]
    hidden_all = lax.all_gather(hidden, "tp", axis=1, tiled=True)
    column_block = lax.all_to_all(
        down_out[0].reshape(unit_rows, tp_count, -1), "tp", split_axis=1, concat_axis=0, tiled=True
    )
    column_block = column_block.reshape(tp_count, unit_rows, -1)
    hidden_blocks = hidden_all.reshape(slot_rows, tp_count, unit_rows)
    partial_value = jnp.einsum(
        "sju,jud->sjd", hidden_blocks, column_block, preferred_element_type=jnp.float32
    ).astype(jnp.bfloat16)
    expert_out = jnp.sum(partial_value, axis=1, dtype=jnp.float32).astype(jnp.bfloat16)
    returned = lax.all_to_all(
        expert_out.reshape(fs_count, capacity, -1), "fs", split_axis=0, concat_axis=0, tiled=True
    )
    returned = returned.reshape(fs_count * capacity, -1)
    picked = returned[slots].reshape(tok_rows, top, -1)
    share = route_weight / jnp.sum(route_weight, axis=1, keepdims=True)
    mixed = jnp.sum(share[:, :, None] * picked.astype(jnp.float32), axis=1).astype(jnp.bfloat16)
    return (gate_out, up_out, down_out, mixed)


MESH = pl.DeviceIdType.MESH
VMEM_BYTES = 67043328


def flip(index, mask):
    other = index
    bit = 1
    while bit <= mask:
        if mask & bit:
            other = other + (1 - 2 * lax.rem(lax.div(index, bit), 2)) * bit
        bit *= 2
    return other


def serve_kernel(
    fs, tp, cap,
    routes_ref, rw_ref, gain_ref, tokens_hbm, gw_hbm, uw_hbm, dw_hbm,
    gat, upw, dn, r, rc, picks_ref, share_ref,
    tokens_ref, gw, uw, dw, gsend, usend, dsend,
    psend, fsend, ftoks, rsend, froutes, ssend, fshares, x, n, h, wd, y, fpicks, fweights, col, whole,
    load_sem,
    out, w_r, t_r, p_r, xf_r, h_r, wd_r, y_s, y_r, met, c_r, m_r,
):
    me = lax.axis_index("fs")
    mt = lax.axis_index("tp")
    toks, cols = tokens_ref.shape
    rows = gw.shape[1]
    units = gw.shape[2]
    each = cols // rows
    slots = fs * cap
    half = fs // 2
    side = lax.div(me, half)
    bridge = half | half // 2
    across = flip(me, bridge)
    outer = (me < fs // 4) | (me >= fs - fs // 4)
    near = list(range(half - 1, 0, -1))
    far = [flip(me, i) for i in range(fs - 1, half - 1, -1)]
    homeward = [jnp.where(side == 1, q, fs - 1 - q) for q in range(half)]
    links = [(i, 0) for i in [1 << b for b in range(half.bit_length() - 1)] + [bridge]]
    links += [(0, 1 << b) for b in range(tp.bit_length() - 1)]
    direct = [1] + list(range(2, tp, 2))
    relayed = list(range(2, tp, 2))

    loads = [
        pltpu.make_async_copy(src, dst, load_sem.at[k])
        for k, (src, dst) in enumerate(
            ((gw_hbm, gw), (uw_hbm, uw), (dw_hbm, dw), (tokens_hbm, tokens_ref))
        )
    ]
    for load in loads[3:] + loads[:3]:
        load.start()

    barrier = pltpu.get_barrier_semaphore()

    def greet(sem):
        for i, j in links:
            pl.semaphore_signal(
                sem, inc=1, device_id=(flip(me, i), flip(mt, j)), device_id_type=MESH
            )

    r[...] = jnp.zeros(r.shape, r.dtype)
    rc[...] = jnp.zeros(rc.shape, rc.dtype)
    greet(barrier)

    def remote(src, dst, s, d, device):
        return pltpu.make_async_remote_copy(
            src_ref=src, dst_ref=dst, send_sem=s, recv_sem=d, device_id=device, device_id_type=MESH
        )

    def drain(ref, sem):
        pltpu.make_async_copy(ref, ref, sem).wait()

    def send(*args):
        copy = remote(*args)
        copy.start()
        return copy

    earlier = lax.broadcasted_iota(jnp.int32, (toks, toks), 0) < lax.broadcasted_iota(
        jnp.int32, (toks, toks), 1
    )
    earlier = jnp.where(earlier, 1.0, 0.0).astype(jnp.bfloat16)
    place = lax.broadcasted_iota(jnp.int32, (cap, toks), 0).astype(jnp.float32)

    def ranks(one, two, lowest):
        expert = lax.broadcasted_iota(jnp.int32, (fs, toks), 0) + lowest
        member = (expert == one) | (expert == two)
        rank = jnp.dot(
            jnp.where(member, 1.0, 0.0).astype(jnp.bfloat16), earlier,
            preferred_element_type=jnp.float32,
        )
        return jnp.where(member, rank, -1.0)

    def pack(rank, rows_of, into):
        for e in range(half):
            hit = jnp.where(place == rank[e:e + 1, :], 1.0, 0.0).astype(jnp.bfloat16)
            into[e] = jnp.dot(hit, rows_of, preferred_element_type=jnp.float32).astype(jnp.bfloat16)

    first, second = routes_ref[0:1, :], routes_ref[1:2, :]
    rsend[0:2, :] = routes_ref[...]
    ssend[0:2, :] = rw_ref[...] / (rw_ref[0:1, :] + rw_ref[1:2, :])
    rank = ranks(first, second, side * half)
    loads[3].wait()
    pack(rank, tokens_ref[...], psend)
    x[mt, me] = psend[lax.rem(me, half)]

    pl.semaphore_wait(barrier, len(links))
    greet(met.at[0])
    crossing = [
        send(rsend, froutes, out.at[0], t_r.at[0], (across, mt)),
        send(ssend, fshares, out.at[0], t_r.at[2], (across, mt)),
        send(tokens_ref, ftoks, out.at[0], t_r.at[1], (across, mt)),
    ]
    pl.semaphore_wait(met.at[0], len(links))
    greet(met.at[1])
    pl.semaphore_wait(met.at[1], len(links))

    def dispatch(buf, block, base):
        for i in near:
            peer = flip(me, i)
            send(
                buf.at[lax.rem(peer, half)], x.at[mt, block], out.at[0], p_r.at[base],
                (peer, mt),
            )

    def forward(i, apart):
        block = flip(me, i ^ bridge if apart else i)
        for j in direct:
            send(
                x.at[mt, block], x.at[mt, block], out.at[0], xf_r.at[j - 1, apart], (me, flip(mt, j))
            )

    dispatch(psend, me, 0)
    forward(0, 0)

    gain = jnp.broadcast_to(gain_ref[...], (units, rows)).T
    placed = {}
    held = {4: []}
    for k, (raw, buf, dst) in enumerate(((gw, gsend, gat), (uw, usend, upw), (dw, dsend, dn))):
        loads[k].wait()
        for e in range(fs):
            buf[e] = (gain * raw[e] if k < 2 else raw[e]).astype(jnp.bfloat16)
        target = dst.at[me] if k < 2 else dst.at[:, pl.ds(pl.multiple_of(me * rows, rows), rows)]
        held[k] = []
        base = 0 if k == 0 else 2 if k == 1 else 3 + half
        for i in near:
            peer = flip(me, i)
            placed[k, i] = remote(buf.at[peer], target, out.at[0], w_r.at[base], (peer, mt))
            if k == 0:
                placed[k, i].start()
        for v, peer in enumerate(far):
            arrived = base + 1 + (v if k else 0)
            copy = remote(buf.at[peer], target, out.at[0], w_r.at[arrived], (peer, mt))
            if k < 2:
                pl.when(jnp.logical_not(outer))(copy.start)
            else:
                pl.when(jnp.logical_not(outer) & (lax.rem(mt, 2) == 0))(copy.start)
                held[4].append((jnp.logical_not(outer) & (lax.rem(mt, 2) == 1), copy))
            held[k].append((outer, copy))
        if k < 2:
            dst[me] = buf[me]
        else:
            dst[:, pl.ds(pl.multiple_of(me * rows, rows), rows)] = buf[me]

    def release(k):
        for when, copy in held[k]:
            pl.when(when)(copy.start)

    for copy in crossing:
        copy.wait_recv()
    pack(ranks(froutes[0:1, :], froutes[1:2, :], side * half), ftoks[...], fsend)
    x[mt, across] = fsend[lax.rem(me, half)]
    dispatch(fsend, across, 1)
    forward(0, 1)
    for k in (2, 1):
        for i in near:
            placed[k, i].start()
    release(0)
    release(1)
    for apart in range(2):
        drain(psend.at[pl.ds(0, half - 1)], p_r.at[apart])
        for i in near:
            forward(i, apart)

    for v in range(2):
        first_block = pl.multiple_of((1 - side if v else side) * half, half)
        for j in relayed:
            landed = x.at[flip(mt, j), pl.ds(first_block, half)]
            drain(landed, xf_r.at[j - 1, v])
            send(landed, landed, out.at[0], xf_r.at[j, v], (me, flip(mt, 1)))

    def gather(apart, steps):
        for v in steps:
            if apart:
                drain(dsend.at[0], w_r.at[4 + half + v])
            elif v == 0:
                drain(dsend.at[pl.ds(0, half - 1)], w_r.at[3 + half])
            piece = far[v] if apart else flip(me, v)
            owner, part = lax.rem(piece, tp), lax.div(piece, tp)
            block = dn.at[:, pl.ds(pl.multiple_of(piece * rows, rows), rows)]
            landing = wd_r.at[apart]
            stays = pltpu.make_async_copy(block, wd.at[mt, part], landing)
            goes = remote(block, wd.at[mt, part], out.at[0], landing, (me, owner))
            pl.when(owner == mt)(stays.start)
            pl.when(owner != mt)(goes.start)

    def choose(one, two, lowest, experts, shares, picks, weights):
        rank = ranks(one, two, lowest)
        hits = [jnp.where(place == rank[e:e + 1, :], 1.0, 0.0) for e in range(experts)]
        for k, named in enumerate((one, two)):
            picked = jnp.concatenate(
                [jnp.where(named == e + lowest, hits[e], 0.0) for e in range(experts)], axis=0
            )
            picks[k] = picked.T.astype(jnp.bfloat16)
            weights[k] = jnp.broadcast_to(shares[k:k + 1, :], (toks, toks)).T

    choose(first, second, 0, fs, ssend, picks_ref, share_ref)
    choose(
        froutes[0:1, :], froutes[1:2, :], side * half, half, fshares, fpicks, fweights
    )

    for v in range(2):
        for j in range(1, tp, 2):
            drain(x.at[0, pl.ds(0, half)], xf_r.at[j - 1, v])

    for s in range(fs):
        total = jnp.zeros((cap, 1), jnp.float32)
        for j in range(tp):
            value = x[j, s].astype(jnp.float32)
            total = total + jnp.sum(value * value, axis=-1, keepdims=True)
        scale = lax.rsqrt(total / (tp * cols) + 1e-06)
        for j in range(tp):
            normed = (x[j, s].astype(jnp.float32) * scale).astype(jnp.bfloat16)
            for part in range(each):
                n[j * each + part, s * cap:(s + 1) * cap] = normed[:, part * rows:(part + 1) * rows]

    def activate(k, dst):
        base = 0 if k == 0 else 2
        drain(dst.at[pl.ds(0, half - 1)], w_r.at[base])
        pieces = [me] + [flip(me, i) for i in near] + far
        act = jnp.zeros((slots, units), jnp.float32)
        for v, piece in enumerate(pieces):
            if k == 0 and v == half:
                drain(dst.at[pl.ds(0, half)], w_r.at[base + 1])
            if k == 1 and v >= half:
                drain(dst.at[0], w_r.at[base + 1 + v - half])
            act = act + jnp.dot(n[piece], dst[piece], preferred_element_type=jnp.float32)
        return act

    release(4)
    gate_act = activate(0, gat)
    gate_act = gate_act / (1.0 + jnp.exp(-gate_act))
    gather(0, range(half))
    up_act = activate(1, upw)
    h[mt] = (gate_act * up_act).astype(jnp.bfloat16)
    shared = {j: send(h.at[mt], h.at[mt], out.at[0], h_r.at[j - 1], (me, flip(mt, j))) for j in direct}
    release(2)
    for j in relayed:
        shared[j].wait_recv()
        source = flip(mt, j)
        shared[j + 1] = send(
            h.at[source], h.at[source], out.at[0], h_r.at[j], (me, flip(mt, 1))
        )

    moves = []

    def give_back(late):
        first_part = (1 - side if late else side) * (each // 2)
        drain(wd.at[:, pl.ds(0, each // 2)], wd_r.at[late])
        for q in range(each // 2):
            part = first_part + q
            result = jnp.zeros((slots, rows), jnp.float32)
            for j in range(tp):
                term = jnp.dot(h[j], wd[j, part], preferred_element_type=jnp.float32)
                result = result + term.astype(jnp.bfloat16).astype(jnp.float32)
            v = late * (each // 2) + q
            y[v] = result.astype(jnp.bfloat16).reshape(fs, cap, rows)
            piece = part * tp + mt
            home, slot = lax.div(piece, each), lax.rem(piece, each)
            peer = flip(me, near[-1])
            send(y.at[v, peer], r.at[slot, me], out.at[0], y_r.at[0], (peer, home))
            if late:
                for peer in homeward:
                    send(y.at[v, peer], r.at[slot, me], out.at[0], y_r.at[1], (peer, home))
            else:
                mine = lax.rem(me, half)
                for i in near:
                    peer = flip(me, i)
                    send(y.at[v, flip(me, i ^ bridge)], col.at[q, mine], out.at[0], c_r.at[0], (peer, mt))
                col[q, mine] = y[v, across]
            for i in near[:-1]:
                peer = flip(me, i)
                send(y.at[v, peer], r.at[slot, me], out.at[0], y_r.at[0], (peer, home))
            stays = pltpu.make_async_copy(y.at[v, me], r.at[slot, me], y_r.at[0])
            goes = remote(y.at[v, me], r.at[slot, me], y_s.at[v], y_r.at[0], (me, home))
            pl.when(home == mt)(stays.start)
            pl.when(home != mt)(goes.start)
            moves.append((home != mt, goes))

    def combine():
        waiting = []
        for _ in range(each // 2):
            drain(col.at[0, pl.ds(0, half - 1)], c_r.at[0])
        for q in range(each // 2):
            back = col[q].reshape(half * cap, rows)
            total = jnp.zeros((toks, rows), jnp.float32)
            for k in range(2):
                term = jnp.dot(fpicks[k], back, preferred_element_type=jnp.float32)
                total = total + fweights[k][:, 0:1] * term
            whole[q] = total.astype(jnp.bfloat16)
            piece = (side * (each // 2) + q) * tp + mt
            home, slot = lax.div(piece, each), lax.rem(piece, each)
            copy = remote(whole.at[q], rc.at[slot], out.at[0], m_r.at[0], (across, home))
            copy.start()
        return waiting

    for j, copy in shared.items():
        if j % 2:
            copy.wait_recv()
    give_back(0)
    gather(1, range(half))
    held[3] = combine()
    release(3)
    give_back(1)

    drain(r.at[:, pl.ds(0, half)], y_r.at[0])
    alike = lax.div(mt, tp // 2) == side

    @pl.when(alike)
    def _():
        drain(r.at[:, pl.ds(0, half)], y_r.at[1])

    @pl.when(jnp.logical_not(alike))
    def _():
        drain(rc, m_r.at[0])

    for copy in crossing:
        copy.wait_send()
    for k, buf in enumerate((gsend, usend, dsend)):
        drain(buf.at[pl.ds(0, fs - 1)], out.at[0])
    for _ in range(2):
        drain(psend.at[pl.ds(0, half - 1)], out.at[0])
    for _ in range(tp - 1):
        drain(x.at[0], out.at[0])
    drain(h.at[pl.ds(0, tp - 1)], out.at[0])
    for _ in range(tp - 1):
        drain(wd.at[0], out.at[0])
    drain(y.at[pl.ds(0, each // 2), pl.ds(0, half - 1)], out.at[0])
    drain(y.at[pl.ds(0, each // 2), pl.ds(0, fs - 1)], out.at[0])
    drain(y.at[pl.ds(0, each // 2), pl.ds(0, half - 1)], out.at[0])
    drain(whole, out.at[0])
    for away, goes in moves:
        pl.when(away)(goes.wait_send)


def mix_kernel(gat, upw, dn, r, rc, picks_ref, share_ref, gate_hbm, up_hbm, down_hbm, mixed_hbm, mixed, sem):
    outs = [
        pltpu.make_async_copy(src, dst, sem.at[k])
        for k, (src, dst) in enumerate(
            ((gat, gate_hbm), (upw, up_hbm), (dn, down_hbm), (mixed, mixed_hbm))
        )
    ]
    for copy in outs[:3]:
        copy.start()
    each, fs, cap, rows = r.shape
    for slot in range(each):
        back = r[slot].reshape(fs * cap, rows)
        total = rc[slot].astype(jnp.float32)
        for k in range(2):
            term = jnp.dot(picks_ref[k], back, preferred_element_type=jnp.float32)
            total = total + share_ref[k][:, 0:1] * term
        mixed[:, slot * rows:(slot + 1) * rows] = total.astype(jnp.bfloat16)
    outs[3].start()
    for copy in outs:
        copy.wait()


def fused(tokens, routes, route_weight, gain, gate_weight, up_weight, down_weight):
    fs = lax.axis_size("fs")
    tp = lax.axis_size("tp")
    toks, cols = tokens.shape
    top = routes.shape[1]
    cap = capacity_of(toks, top, fs)
    rows, units = gate_weight.shape[1:]
    each = cols // rows
    slots = fs * cap
    bf, f32 = jnp.bfloat16, jnp.float32
    hbm, vmem = pl.BlockSpec(memory_space=pltpu.HBM), pl.BlockSpec(memory_space=pltpu.VMEM)
    dma = pltpu.SemaphoreType.DMA
    kept = 2 * (3 * fs * rows * units + slots * cols + toks * cols + top * toks * slots) + 4 * top * toks * toks
    landed = pl.pallas_call(
        functools.partial(serve_kernel, fs, tp, cap),
        out_shape=(
            pltpu.VMEM((fs, rows, units), bf),
            pltpu.VMEM((fs, rows, units), bf),
            pltpu.VMEM((units, fs * rows), bf),
            pltpu.VMEM((each, fs, cap, rows), bf),
            pltpu.VMEM((each, toks, rows), bf),
            pltpu.VMEM((top, toks, slots), bf),
            pltpu.VMEM((top, toks, toks), f32),
        ),
        in_specs=[vmem] * 3 + [hbm] * 4,
        out_specs=(vmem,) * 7,
        scratch_shapes=[
            pltpu.VMEM((toks, cols), bf),
            pltpu.VMEM((fs, rows, units), f32),
            pltpu.VMEM((fs, rows, units), f32),
            pltpu.VMEM((fs, units, rows), f32),
            pltpu.VMEM((fs, rows, units), bf),
            pltpu.VMEM((fs, rows, units), bf),
            pltpu.VMEM((fs, units, rows), bf),
            pltpu.VMEM((fs // 2, cap, cols), bf),
            pltpu.VMEM((fs // 2, cap, cols), bf),
            pltpu.VMEM((toks, cols), bf),
            pltpu.VMEM((8, toks), jnp.int32),
            pltpu.VMEM((8, toks), jnp.int32),
            pltpu.VMEM((8, toks), f32),
            pltpu.VMEM((8, toks), f32),
            pltpu.VMEM((tp, fs, cap, cols), bf),
            pltpu.VMEM((fs, slots, rows), bf),
            pltpu.VMEM((tp, slots, units), bf),
            pltpu.VMEM((tp, each, units, rows), bf),
            pltpu.VMEM((each, fs, cap, rows), bf),
            pltpu.VMEM((top, toks, slots // 2), bf),
            pltpu.VMEM((top, toks, toks), f32),
            pltpu.VMEM((each // 2, fs // 2, cap, rows), bf),
            pltpu.VMEM((each // 2, toks, rows), bf),
            dma((4,)),
            dma((1,)), dma((fs + 4,)), dma((3,)), dma((2,)), dma((tp - 1, 2)), dma((tp - 1,)),
            dma((2,)), dma((each,)), dma((2,)),
            pltpu.SemaphoreType.REGULAR((2,)),
            dma((1,)), dma((1,)),
        ],
        compiler_params=pltpu.CompilerParams(
            collective_id=0, has_side_effects=True, vmem_limit_bytes=VMEM_BYTES - kept - 2**16
        ),
        name="serve",
    )(routes.T, route_weight.T, gain.reshape(1, -1), tokens, gate_weight, up_weight, down_weight)
    gate, up, down, mixed = pl.pallas_call(
        mix_kernel,
        out_shape=(
            jax.ShapeDtypeStruct((fs, rows, units), bf),
            jax.ShapeDtypeStruct((fs, rows, units), bf),
            jax.ShapeDtypeStruct((units, fs * rows), bf),
            jax.ShapeDtypeStruct((toks, cols), bf),
        ),
        in_specs=[vmem] * 7,
        out_specs=(hbm,) * 4,
        scratch_shapes=[pltpu.VMEM((toks, cols), bf), dma((4,))],
        compiler_params=pltpu.CompilerParams(vmem_limit_bytes=16 * 2**20),
        name="mix",
    )(*landed)
    return (
        gate.reshape(1, fs * rows, units),
        up.reshape(1, fs * rows, units),
        down[None],
        mixed,
    )


def capacity_of(tok_rows, top, fs_count):
    return min(tok_rows, max(2, 3 * tok_rows * top // (2 * fs_count)))


def one_kernel(fs, tp, toks, top, experts, rows, units, cols):
    cap = capacity_of(toks, top, fs)
    powers = fs & (fs - 1) == 0 and tp & (tp - 1) == 0 and fs >= 4 and tp >= 2
    small = fs <= 16 and tp <= 8 and top == 2 and experts == fs
    tiled = cap % 16 == 0 and rows % 128 == 0 and units % 128 == 0 and toks % 128 == 0
    return powers and small and tiled and cols % (2 * rows) == 0 and fs * rows == tp * cols


def program(*args):
    tokens, routes, gate_weight = args[0], args[1], args[4]
    experts, rows, units = gate_weight.shape
    if one_kernel(
        lax.axis_size("fs"), lax.axis_size("tp"), tokens.shape[0], routes.shape[1],
        experts, rows, units, tokens.shape[1],
    ):
        return fused(*args)
    return local(*args)


def solution(mesh):
    in_specs = (
        P("fs", "tp"),
        P("fs", None),
        P("fs", None),
        P("fs"),
        P(None, "fs", "tp"),
        P(None, "fs", "tp"),
        P(None, "tp", "fs"),
    )
    out_specs = (P("fs", None, "tp"), P("fs", None, "tp"), P("fs", "tp", None), P("fs", "tp"))
    return jax.shard_map(program, mesh=mesh, in_specs=in_specs, out_specs=out_specs, check_vma=False)
```
